32 devices in a mesh: grp: 2 (over x), ep: 4 (over y, core), tp: 4 (over z).
Axes of the slice: x: 2, y: 2, z: 4, core: 2. Of those that a mesh axis runs over, the one named last changes fastest.
Arguments:
- tokens: bfloat16 [512, 2048], P(('grp', 'ep')), parts along dimension 0, may hold values from -6 to 6
- routing: int32 [512, 4], P(('grp', 'ep')), parts along dimension 0, may hold values from 0 to 7, all different within a row; in each aligned block of 64 rows (0 to 63, 64 to 127, ...) at most 64 rows name the same one
- route_weight: float32 [512, 4], P(('grp', 'ep')), parts along dimension 0, may hold values from 0.1 to 1
- norm_gain: float32 [2048], replicated, may hold values from 0.1 to 1.9
- gate_weight: bfloat16 [8, 2048, 2048], P('ep', None, 'tp'), may hold values from -2.1213203 to 2.1213203
- up_weight: bfloat16 [8, 2048, 2048], P('ep', None, 'tp'), may hold values from -2.1213203 to 2.1213203
- down_weight: bfloat16 [8, 2048, 2048], P('ep', 'tp'), may hold values from -3.9774756 to 3.9774756
- out_gain: float32 [2048], P('tp'), may hold values from 0.1 to 1.9
Outputs:
- layer_output: bfloat16 [512, 2048], P(('grp', 'ep'), 'tp'), parts along dimension 0
The draws below stay inside these ranges and needn't reach their ends.
There are 2 independent parts, one for each index of `grp`. The reference program is written for one: setup_inputs(seed, part) draws one part's arguments, and reference() takes and returns one part's arrays. A program takes and returns all parts, laid end to end along the dimension named above; an argument that names none is the same for every part. Nothing has to cross between parts.
Inputs may be any that keep to these rules, and one draw needn't show every extreme that they name: `routing`: each row names 4 different experts; among the 64 rows of one index of ep no expert is named more than 64 times, and in some such blocks one expert is named exactly 64 times.
All inputs are finite; a program needn't handle non-finite values.
Results may differ from the reference program's by a relative error of at most 0.017.
Values may be sent and summed in bfloat16 or wider, within the bound.
A program may use at most 64 MiB of HBM per device.

```python
import math
import jax
import jax.numpy as jnp
import numpy as np
from jax import lax

D = 2048
FF = 2048
TOPK = 4
TOK_DEV = 64
EXPERTS = 8
TOKENS = 256
CAP = 64
EXPERT_ROWS = 256
FF_DEV = 512
N_EP = 4
N_TP = 4


def projection_draw(key, salt_value):
    base = jax.random.fold_in(key, salt_value)
    entry_key, column_key = jax.random.split(base, 2)
    entries = jax.random.truncated_normal(entry_key, -6.0, 6.0, (EXPERTS, D, FF), jnp.float32)
    column = jnp.exp(jax.random.uniform(column_key, (EXPERTS, 1, FF), jnp.float32, 0.0, math.log(8.0)))
    return (entries * column * D ** (-0.5)).astype(jnp.bfloat16)


def draw_gate_weight(key, part):
    return projection_draw(key, 101)


def draw_up_weight(key, part):
    return projection_draw(key, 202)


def draw_down_weight(key, part):
    base = jax.random.fold_in(key, 303)
    entry_key, column_key = jax.random.split(base, 2)
    ramp = jnp.arange(D, dtype=jnp.float32) / D
    entries = jax.random.truncated_normal(entry_key, -6.0, 6.0, (EXPERTS, FF, D), jnp.float32)
    rising = jnp.exp(math.log(4.0) * ramp)
    column = rising[None, None, :] * jnp.exp(jax.random.uniform(column_key, (EXPERTS, 1, D), jnp.float32, 0.0, math.log(3.0)))
    return (entries * column * FF ** (-0.5)).astype(jnp.bfloat16)


def block_levels(rng, extent, cuts, low, largest):
    loudness, own = 1.0, jax.random.fold_in(rng, 6)
    for dim, blocks in cuts:
        heights = jnp.exp(jax.random.uniform(jax.random.fold_in(own, dim), (blocks,), jnp.float32, low / len(cuts), largest / len(cuts)))
        loudness = loudness * jnp.repeat(heights, extent[dim] // blocks).reshape([-1 if axis == dim else 1 for axis in range(len(extent))])
    return loudness


def assign_block(stream_key, own, number, rows, count, top, bound, slope):
    sequence = jax.random.permutation(stream_key, count)
    crowded, usual = shares(count, rows * top, bound, slope, True), shares(count, rows * top, bound, slope, False)
    places = jnp.arange(count)

    def named(lengths, rotation):
        used = int((lengths > 0).sum())
        fixed = max(1, used // 4)
        moved = fixed + (places - fixed + rotation * (used - fixed)) % max(1, count - fixed)
        return jnp.zeros((count,), jnp.int32).at[sequence[jnp.where(places < fixed, places, moved)]].set(jnp.asarray(lengths, jnp.int32))

    lengths = jnp.where(number % 4 == 0, named(crowded, number // 4), named(usual, number - number // 4 - 1))
    mixed = jax.random.permutation(jax.random.fold_in(own, 3), count)
    giver, receiver = mixed[0:count // 2 * 2:2], mixed[1:count // 2 * 2:2]
    margin = jnp.minimum(lengths[giver] - 1, bound - lengths[receiver]) // 2
    margin = jnp.where((giver == sequence[0]) | (receiver == sequence[0]) | (lengths[receiver] == 0), 0, jnp.maximum(margin, 0))
    moved = jax.random.randint(jax.random.fold_in(own, 4), (count // 2,), 0, 1 << 20) % (margin + 1)
    lengths = lengths.at[giver].add(-moved).at[receiver].add(moved)
    members = jnp.searchsorted(jnp.cumsum(lengths), jnp.arange(rows * top), side="right").astype(jnp.int32)
    table = members.reshape(top, rows).T
    table = table[jax.random.permutation(jax.random.fold_in(own, 1), rows)]
    rotation = jax.random.randint(jax.random.fold_in(own, 2), (rows, 1), 0, top)
    return jnp.take_along_axis(table, (jnp.arange(top)[None, :] + rotation) % top, axis=1)


def shares(number_of, total, most, slope, full):
    portions = [(1 << 20) // math.isqrt(rank ** slope) + 1 for rank in range(1, number_of + 1)]
    largest = most if full else min(most, max(-(-total // number_of), total * portions[0] // sum(portions)))
    least = 1 if total - largest >= number_of - 1 else 0
    given, surplus = [largest] + [least] * (number_of - 1), total - largest - least * (number_of - 1)
    while surplus > 0:
        movable = [i for i in range(1, number_of) if given[i] < largest] or [i for i in range(1, number_of) if given[i] < most]
        pool, remaining = sum([portions[i] for i in movable]), surplus
        for i in movable:
            extra = min(most - given[i], max(1, remaining * portions[i] // pool), surplus)
            given[i] = given[i] + extra
            surplus = surplus - extra
    return np.array(given)


def gaussian(own_key, extent, scale, most, shards=(), kind=jnp.bfloat16):
    drawn = scale * jax.random.normal(own_key, extent, jnp.float32)
    if shards:
        drawn = drawn * block_levels(own_key, extent, shards, -0.22, 0.18)
    return jnp.clip(drawn, -most, most).astype(kind)


def setup_inputs(seed: int = 0, part: int = 0) -> dict:
    seeds = jax.random.split(jax.random.key(seed), 9)
    part_splits = jax.random.split(jax.random.fold_in(seeds[8], part), 9)
    tokens = gaussian(part_splits[0], (TOKENS, D), 1.0, 6.0, ((0, 4),))
    routing_keys = jax.random.split(jax.random.fold_in(part_splits[1], 1), TOKENS // TOK_DEV)
    routing_turns = jax.random.permutation(jax.random.fold_in(part_splits[1], 3), TOKENS // TOK_DEV)
    routing = jax.vmap(lambda own, number: assign_block(jax.random.fold_in(part_splits[1], 2), own, number, TOK_DEV, EXPERTS, TOPK, CAP, 2))(routing_keys, routing_turns).reshape((TOKENS, TOPK))
    route_weight = jnp.clip(jnp.exp(math.log(1.0) - 2.3025851 * jax.random.uniform(part_splits[2], (TOKENS, TOPK), jnp.float32) ** block_levels(part_splits[2], (TOKENS, TOPK), ((0, 4),), -0.2, 0.2)), 0.1, 1.0)
    norm_gain = jnp.clip(1.0 + 0.18 * jax.random.normal(seeds[3], (D,), jnp.float32), 0.1, 1.9)
    gate_weight = draw_gate_weight(jax.random.fold_in(seeds[8], 71), part)
    up_weight = draw_up_weight(jax.random.fold_in(seeds[8], 71), part)
    down_weight = draw_down_weight(jax.random.fold_in(seeds[8], 71), part)
    out_gain = jnp.clip(1.0 + 0.18 * jax.random.normal(seeds[7], (D,), jnp.float32), 0.1, 1.9)
    return {"tokens": tokens, "routing": routing, "route_weight": route_weight, "norm_gain": norm_gain, "gate_weight": gate_weight, "up_weight": up_weight, "down_weight": down_weight, "out_gain": out_gain}


LIMIT = 7.0
ALPHA = 1.702
EPS = 1e-06

def slot_ranks(routing):
    assign_count = TOK_DEV * TOPK
    blocks = routing.reshape(N_EP, assign_count)
    same_expert = blocks[:, :, None] == blocks[:, None, :]
    position = jnp.arange(assign_count, dtype=jnp.int32)
    earlier = position[None, :] < position[:, None]
    counted = jnp.where(same_expert & earlier[None, :, :], 1, 0).astype(jnp.int32)
    return lax.optimization_barrier(jnp.sum(counted, axis=2)).astype(jnp.int32).reshape(TOKENS, TOPK)

def reference(tokens, routing, route_weight, norm_gain, gate_weight, up_weight, down_weight, out_gain):
    scaled = tokens.astype(jnp.float32)
    normed = (scaled * lax.rsqrt(lax.optimization_barrier(jnp.mean(scaled * scaled, axis=-1, keepdims=True)) + EPS) * norm_gain).astype(jnp.bfloat16)
    slot_rank = slot_ranks(routing)
    source = (jnp.arange(TOKENS, dtype=jnp.int32) // TOK_DEV)[:, None]
    buffer_row = (source * CAP + slot_rank).astype(jnp.int32)
    buffer = jnp.zeros((EXPERTS, EXPERT_ROWS, D), jnp.bfloat16)
    repeated = jnp.broadcast_to(normed[:, None, :], (TOKENS, TOPK, D))
    buffer = buffer.at[routing, buffer_row].set(repeated)

    def expert(operands):
        expert_rows, gate_block, up_block, down_block = operands
        gate_act = jnp.minimum(jnp.dot(expert_rows, gate_block, preferred_element_type=jnp.float32), LIMIT)
        up_act = jnp.clip(jnp.dot(expert_rows, up_block, preferred_element_type=jnp.float32), -LIMIT, LIMIT)
        hidden = ((up_act + 1.0) * gate_act * jax.nn.sigmoid(ALPHA * gate_act)).astype(jnp.bfloat16)
        pieces = hidden.reshape(EXPERT_ROWS, N_TP, FF_DEV).astype(jnp.float32)
        blocks = down_block.reshape(N_TP, FF_DEV, D).astype(jnp.float32)
        partial_sums = jnp.einsum('rnf,nfd->nrd', pieces, blocks).astype(jnp.bfloat16)
        return lax.optimization_barrier(jnp.sum(partial_sums.astype(jnp.float32), axis=0)).astype(jnp.bfloat16)
    expert_out = lax.map(expert, (buffer, gate_weight, up_weight, down_weight))
    picked = expert_out[routing, buffer_row].astype(jnp.float32)
    expert_mix = lax.optimization_barrier(jnp.sum(route_weight[:, :, None] * picked, axis=1))
    square_mean = lax.optimization_barrier(jnp.mean(expert_mix * expert_mix, axis=-1, keepdims=True))
    return (expert_mix * lax.rsqrt(square_mean + EPS) * out_gain).astype(jnp.bfloat16)
```

```python
import functools

import jax
import jax.numpy as jnp
from jax import lax
from jax.experimental import pallas as pl
from jax.experimental.pallas import tpu as pltpu
from jax.sharding import PartitionSpec as P

LIMIT = 7.0
ALPHA = 1.702
EPS = 1e-06
LANES = 128
PIECES = 8
SIDE = 2
CHUNKS = ((0, 4), (4, 8))
MESH = pl.DeviceIdType.MESH
BF16 = jnp.bfloat16
F32 = jnp.float32


def kernel(
    ep_size,
    tp_size,
    tok_hbm,
    route_hbm,
    weight_hbm,
    gain_hbm,
    out_gain_hbm,
    gate_hbm,
    up_hbm,
    down_hbm,
    out_ref,
    tok_ref,
    route_ref,
    weight_ref,
    gain_ref,
    out_gain_ref,
    rows,
    codes,
    gu_buf,
    down_buf,
    acc,
    hidden,
    core_out,
    core_in,
    core_sum,
    own_sum,
    near_sum,
    late_sum,
    chip_out,
    chip_in,
    early_out,
    early_in,
    late_out,
    late_in,
    back_out,
    back_in,
    feat_out,
    feat_in,
    square_out,
    square_in,
    small_sem,
    load_sem,
    ready,
    sent_sem,
    pair_recv,
    code_recv,
    chip_recv,
    side_recv,
    fwd_recv,
    core_recv,
    red_recv,
    early_recv,
    late_recv,
    back_recv,
    feat_recv,
    sq_recv,
):
    me, tp = lax.axis_index("ep"), lax.axis_index("tp")
    core = lax.rem(me, 2)
    chip = lax.div(me, 2)
    odd = lax.rem(tp, 2)
    partner = me + 1 - 2 * core
    beside = {"tp": tp + 1 - 2 * odd}
    chips = ep_size // 2
    toks, width = tok_ref.shape
    experts, _, _, ff = gu_buf.shape
    out_width = width // tp_size
    cut = out_width // 2
    depth = width // PIECES
    direct = PIECES - SIDE

    def chip_at(step):
        return lax.rem(chip + step, chips)

    def tp_at(step):
        return lax.rem(tp + step, tp_size)

    def send(src, dst, send_sem, recv_sem, device):
        return pltpu.make_async_remote_copy(
            src_ref=src,
            dst_ref=dst,
            send_sem=send_sem,
            recv_sem=recv_sem,
            device_id=device,
            device_id_type=MESH,
        )

    sent = []

    def start(src, dst, recv_sem, device):
        copy = send(src, dst, sent_sem, recv_sem, device)
        copy.start()
        sent.append(copy)

    def arrived(slot, sem):
        send(slot, slot, sent_sem, sem, {"ep": partner}).wait_recv()

    def tell(sem):
        @pl.when(tp > 0)
        def _():
            pl.semaphore_signal(sem, inc=1, device_id={"tp": tp - 1}, device_id_type=MESH)

        @pl.when(tp < tp_size - 1)
        def _():
            pl.semaphore_signal(sem, inc=1, device_id={"tp": tp + 1}, device_id_type=MESH)

    beside_count = lax.div(tp + tp_size - 1, tp_size) + lax.div(2 * tp_size - 2 - tp, tp_size)

    loads = []
    for e in range(experts):
        loads.append((gate_hbm.at[e], gu_buf.at[e, 0], e))
        loads.append((up_hbm.at[e], gu_buf.at[e, 1], e))
    for e in range(experts):
        loads.append((down_hbm.at[e], down_buf.at[pl.ds(e * ff, ff)], experts))
    loads = [pltpu.make_async_copy(src, dst, load_sem.at[i]) for src, dst, i in loads]

    def loaded(slot, i):
        pltpu.make_async_copy(slot, slot, load_sem.at[i]).wait()

    smalls = (
        (tok_hbm, tok_ref),
        (gain_hbm, gain_ref),
        (route_hbm, route_ref),
        (weight_hbm, weight_ref),
        (out_gain_hbm, out_gain_ref),
    )
    smalls = [
        pltpu.make_async_copy(src, dst, small_sem.at[i]) for i, (src, dst) in enumerate(smalls)
    ]
    barrier = pltpu.get_barrier_semaphore()
    for load in smalls:
        load.start()
    for step in range(1, ep_size):
        pl.semaphore_signal(
            barrier, inc=1, device_id={"ep": lax.rem(me + step, ep_size)}, device_id_type=MESH
        )
    tell(barrier)
    for load in loads:
        load.start()

    for load in smalls[:2]:
        load.wait()
    scaled = tok_ref[...].astype(F32)
    scale = lax.rsqrt(jnp.mean(scaled * scaled, axis=-1, keepdims=True) + EPS)
    scaled = (scaled * scale * gain_ref[...]).astype(BF16)
    for p in range(PIECES):
        rows[me, p] = scaled[:, p * depth : (p + 1) * depth]

    pl.semaphore_wait(barrier, ep_size - 1 + beside_count)

    def piece(slot, j):
        return rows.at[slot, j + odd * (PIECES - 1 - 2 * j)]

    for j in range(direct):
        for step in range(1, chips):
            block = piece(me, j)
            start(block, block, chip_recv.at[step - 1, j], {"ep": 2 * chip_at(step) + core})
        if j == 0:
            start(rows.at[me], rows.at[me], pair_recv, {"ep": partner})
    if tp_size > 2:
        tell(ready.at[0])

    for load in smalls[2:4]:
        load.wait()
    place = lax.broadcasted_iota(jnp.int32, (codes.shape[1], toks), 0)
    placed = jnp.zeros(place.shape, F32)
    for k in range(route_ref.shape[0]):
        placed = placed + jnp.where(place == route_ref[k : k + 1], weight_ref[k : k + 1], 0.0)
    codes[me] = jnp.zeros(codes.shape[1:], F32)
    codes[me, :, :toks] = placed
    start(codes.at[me], codes.at[me], code_recv.at[0], {"ep": partner})
    for step in range(1, chips):
        for other in range(2):
            start(
                codes.at[me],
                codes.at[me],
                code_recv.at[1],
                {"ep": 2 * chip_at(step) + other},
            )

    def mixes(index):
        columns = jnp.concatenate([codes[2 * index + c].T[:toks] for c in range(2)], axis=0)
        lane = lax.broadcasted_iota(jnp.int32, columns.shape, 1)
        return [
            jnp.sum(jnp.where(lane == me * experts + e, columns, 0.0), axis=1, keepdims=True)
            for e in range(experts)
        ]

    def features(index, first, count):
        both = pl.ds(2 * index, 2)
        parts = [rows[both, first + t].reshape(2 * toks, depth) for t in range(count)]
        return jnp.concatenate(parts, axis=1)

    def activate(index, e, gate, up, mix):
        gate = jnp.minimum(gate, LIMIT)
        up = jnp.clip(up, -LIMIT, LIMIT)
        act = (up + 1.0) * gate * jax.nn.sigmoid(ALPHA * gate) * mix
        act = act.astype(BF16).reshape(2, toks, ff)
        hidden[pl.ds(2 * index, 2), :, e * ff : (e + 1) * ff] = act

    def own_expert(e, mix):
        x = features(chip, 0, PIECES)
        loaded(gu_buf.at[e], e)
        gate = jnp.dot(x, gu_buf[e, 0], preferred_element_type=F32)
        up = jnp.dot(x, gu_buf[e, 1], preferred_element_type=F32)
        activate(chip, e, gate, up, mix)

    def other_experts(index, number, mix):
        a, b = CHUNKS[number]
        first = a + odd * (PIECES - a - b)
        x = features(index, first, b - a)
        part = pl.ds(pl.multiple_of(first * depth, depth), (b - a) * depth)
        for e in range(experts):
            sums = []
            for i in range(2):
                total = jnp.dot(x, gu_buf[e, i, part, :], preferred_element_type=F32)
                if number:
                    total = total + acc[e, i]
                sums.append(total)
            if number == len(CHUNKS) - 1:
                activate(index, e, sums[0], sums[1], mix[e])
            else:
                for i in range(2):
                    acc[e, i] = sums[i]

    def forward(j):
        number = [a <= j < b for a, b in CHUNKS].index(True)
        for step in range(1, chips):
            block = piece(2 * chip_at(chips - step) + core, j)
            if j < direct:
                arrived(block, chip_recv.at[step - 1, j])
            else:
                arrived(block, side_recv.at[step - 1, j - direct])
            if j < SIDE:
                start(block, block, side_recv.at[step - 1, SIDE - 1 - j], beside)
            start(block, block, fwd_recv.at[step - 1, number], {"ep": partner})

    order = list(range(tp_size // 2, tp_size)) + list(range(1, tp_size // 2))[::-1] + [0]

    def project(step, k):
        index = chip_at(step)
        both = jnp.concatenate([hidden[2 * index + 1 - core], hidden[2 * index + core]], axis=0)
        columns = pl.ds(pl.multiple_of(tp_at(k) * out_width, out_width), out_width)
        out = jnp.dot(both, down_buf[:, columns], preferred_element_type=F32)
        core_out[step, k] = out[:toks].astype(BF16)
        core_sum[step, k] = out[toks:]
        start(
            core_out.at[step, k], core_in.at[step, k], core_recv.at[step, k], {"ep": partner}
        )

    def crossed(step, k):
        block = core_in.at[step, k]
        arrived(block, core_recv.at[step, k])
        return core_sum[step, k] + block[...].astype(F32)

    def own_chip(k):
        total = crossed(0, k)
        own_sum[k] = total[:, :cut]
        if k:
            early_out[k - 1] = total[:, cut:].astype(BF16)
            start(early_out.at[k - 1], early_in.at[k - 1], early_recv, {"tp": tp_at(k)})
        else:
            near_sum[...] = total[:, cut:]

    def other_chip(step, k):
        total = crossed(step, k)
        slot = step - 1
        chip_out[k, slot] = total[:, :cut].astype(BF16)
        start(
            chip_out.at[k, slot],
            chip_in.at[k, slot],
            red_recv.at[k, slot],
            {"ep": 2 * chip_at(step) + core},
        )
        if k:
            late_out[slot, k - 1] = total[:, cut:].astype(BF16)
            start(
                late_out.at[slot, k - 1],
                late_in.at[slot, k - 1],
                late_recv.at[slot],
                {"tp": tp_at(k)},
            )
        else:
            late_sum[slot] = total[:, cut:]

    arrived(rows.at[partner], pair_recv)
    arrived(codes.at[partner], code_recv.at[0])
    mix = mixes(chip)
    for e in range(experts):
        own_expert(e, mix[e])
    for r in range(tp_size - 2):
        pl.semaphore_wait(ready.at[r], beside_count)
        if r + 1 < tp_size - 2:
            tell(ready.at[r + 1])
    forward(0)
    loaded(down_buf, experts)
    for i, k in enumerate(order):
        project(0, k)
        if i == len(order) // 2 - 1:
            forward(1)
    forward(2)
    for k in order:
        own_chip(k)
    for j in list(range(3, direct)) + list(range(direct, PIECES))[::-1]:
        forward(j)
    if chips > 1:
        arrived(codes.at[pl.ds(0, ep_size - 2)], code_recv.at[1])
    for step in range(1, chips):
        index = chip_at(chips - step)
        mix = mixes(index)
        for number, (a, b) in enumerate(CHUNKS):
            first = a + odd * (PIECES - a - b)
            block = rows.at[2 * index + 1 - core, pl.ds(first, b - a)]
            arrived(block, fwd_recv.at[step - 1, number])
            other_experts(index, number, mix)
        for k in order:
            project(chips - step, k)
        for k in order:
            other_chip(chips - step, k)

    for k in order:
        total = own_sum[k]
        for slot in range(chips - 1):
            block = chip_in.at[k, slot]
            arrived(block, red_recv.at[k, slot])
            total = total + block[...].astype(F32)
        if k:
            feat_out[k - 1] = total.astype(BF16)
            start(feat_out.at[k - 1], feat_in.at[k - 1], feat_recv, {"tp": tp_at(k)})
        else:
            left = total
    for slot in range(chips - 1):
        total = late_sum[slot]
        arrived(late_in.at[slot], late_recv.at[slot])
        for k in range(1, tp_size):
            total = total + late_in[slot, k - 1].astype(F32)
        back_out[slot] = total.astype(BF16)
        start(
            back_out.at[slot],
            back_in.at[slot],
            back_recv,
            {"ep": 2 * chip_at(slot + 1) + core},
        )
    right = near_sum[...]
    arrived(early_in, early_recv)
    for k in range(1, tp_size):
        right = right + early_in[k - 1].astype(F32)
    arrived(feat_in, feat_recv)
    for k in range(1, tp_size):
        left = left + feat_in[k - 1].astype(F32)
    if chips > 1:
        arrived(back_in, back_recv)
    for slot in range(chips - 1):
        right = right + back_in[slot].astype(F32)
    mixed = jnp.concatenate([left, right], axis=1)

    squares = mixed * mixed
    folded = jnp.zeros((toks, LANES), F32)
    for j in range(out_width // LANES):
        folded = folded + squares[:, j * LANES : (j + 1) * LANES]
    wide = square_out.shape[1]
    if wide > toks:
        folded = jnp.concatenate([folded, jnp.zeros((wide - toks, LANES), F32)], axis=0)
    line = jnp.sum(folded.T, axis=0, keepdims=True)
    square_out[...] = jnp.broadcast_to(line, square_out.shape)
    for k in range(1, tp_size):
        start(square_out, square_in.at[k - 1], sq_recv, {"tp": tp_at(k)})
    arrived(square_in, sq_recv)
    for k in range(1, tp_size):
        line = line + square_in[k - 1, 0:1, :]
    total = jnp.broadcast_to(line, (LANES, wide)).T[:toks, :1]
    factor = lax.rsqrt(total / width + EPS)
    smalls[4].wait()
    out_ref[...] = (mixed * factor * out_gain_ref[...]).astype(BF16)
    for copy in sent:
        copy.wait_send()


def on_device(
    tokens, routing, route_weight, norm_gain, gate_weight, up_weight, down_weight, out_gain
):
    toks, width = tokens.shape
    experts, _, ff = gate_weight.shape
    ep_size, tp_size = lax.axis_size("ep"), lax.axis_size("tp")
    chips = ep_size // 2
    wide = pl.cdiv(toks, LANES) * LANES
    out_width = width // tp_size
    cut = out_width // 2
    vmem = pl.BlockSpec(memory_space=pltpu.VMEM)
    hbm = pl.BlockSpec(memory_space=pl.ANY)
    dma = pltpu.SemaphoreType.DMA
    return pl.pallas_call(
        functools.partial(kernel, ep_size, tp_size),
        out_shape=pltpu.VMEM((toks, out_width), BF16),
        in_specs=[hbm] * 8,
        out_specs=vmem,
        scratch_shapes=[
            pltpu.VMEM(tokens.shape, tokens.dtype),
            pltpu.VMEM(routing.shape[::-1], routing.dtype),
            pltpu.VMEM(routing.shape[::-1], F32),
            pltpu.VMEM((1, width), F32),
            pltpu.VMEM((1, out_width), F32),
            pltpu.VMEM((ep_size, PIECES, toks, width // PIECES), BF16),
            pltpu.VMEM((ep_size, pl.cdiv(experts * ep_size, 8) * 8, wide), F32),
            pltpu.VMEM((experts, 2, width, ff), BF16),
            pltpu.VMEM((experts * ff, width), BF16),
            pltpu.VMEM((experts, 2, 2 * toks, ff), F32),
            pltpu.VMEM((ep_size, toks, experts * ff), BF16),
            pltpu.VMEM((chips, tp_size, toks, out_width), BF16),
            pltpu.VMEM((chips, tp_size, toks, out_width), BF16),
            pltpu.VMEM((chips, tp_size, toks, out_width), F32),
            pltpu.VMEM((tp_size, toks, cut), F32),
            pltpu.VMEM((toks, cut), F32),
            pltpu.VMEM((chips - 1, toks, cut), F32),
            pltpu.VMEM((tp_size, chips - 1, toks, cut), BF16),
            pltpu.VMEM((tp_size, chips - 1, toks, cut), BF16),
            pltpu.VMEM((tp_size - 1, toks, cut), BF16),
            pltpu.VMEM((tp_size - 1, toks, cut), BF16),
            pltpu.VMEM((chips - 1, tp_size - 1, toks, cut), BF16),
            pltpu.VMEM((chips - 1, tp_size - 1, toks, cut), BF16),
            pltpu.VMEM((chips - 1, toks, cut), BF16),
            pltpu.VMEM((chips - 1, toks, cut), BF16),
            pltpu.VMEM((tp_size - 1, toks, cut), BF16),
            pltpu.VMEM((tp_size - 1, toks, cut), BF16),
            pltpu.VMEM((8, wide), F32),
            pltpu.VMEM((tp_size - 1, 8, wide), F32),
            dma((5,)),
            dma((experts + 1,)),
            pltpu.SemaphoreType.REGULAR((tp_size - 2,)),
            dma,
            dma,
            dma((2,)),
            dma((chips - 1, PIECES - SIDE)),
            dma((chips - 1, SIDE)),
            dma((chips - 1, len(CHUNKS))),
            dma((chips, tp_size)),
            dma((tp_size, chips - 1)),
            dma,
            dma((chips - 1,)),
            dma,
            dma,
            dma,
        ],
        compiler_params=pltpu.CompilerParams(
            collective_id=0, has_side_effects=True, vmem_limit_bytes=60 * 1024 * 1024
        ),
    )(
        tokens,
        routing.T,
        route_weight.T,
        norm_gain.reshape(1, width),
        out_gain.reshape(1, out_width),
        gate_weight,
        up_weight,
        down_weight,
    )


def solution(mesh):
    in_specs = (
        P(("grp", "ep"), None),
        P(("grp", "ep"), None),
        P(("grp", "ep"), None),
        P(),
        P("ep", None, "tp"),
        P("ep", None, "tp"),
        P("ep", "tp", None),
        P("tp"),
    )
    out_specs = P(("grp", "ep"), "tp")
    return jax.shard_map(
        on_device, mesh=mesh, in_specs=in_specs, out_specs=out_specs, check_vma=False
    )
```

```python
import functools

import jax
import jax.numpy as jnp
from jax import lax
from jax.experimental import pallas as pl
from jax.experimental.pallas import tpu as pltpu
from jax.sharding import PartitionSpec as P

LIMIT = 7.0
ALPHA = 1.702
EPS = 1e-06
LANES = 128
PIECES = 8
SIDE = 2
CHUNKS = ((0, 4), (4, 6), (6, 8))
MESH = pl.DeviceIdType.MESH
BF16 = jnp.bfloat16
F32 = jnp.float32


def kernel(
    ep_size,
    tp_size,
    tok_hbm,
    route_hbm,
    weight_hbm,
    gain_hbm,
    out_gain_hbm,
    gate_hbm,
    up_hbm,
    down_hbm,
    out_ref,
    tok_ref,
    route_ref,
    weight_ref,
    gain_ref,
    out_gain_ref,
    rows,
    codes,
    gu_buf,
    down_buf,
    acc,
    hidden,
    core_out,
    core_in,
    core_sum,
    own_sum,
    near_sum,
    late_sum,
    chip_out,
    chip_in,
    early_out,
    early_in,
    late_out,
    late_in,
    back_out,
    back_in,
    feat_out,
    feat_in,
    square_out,
    square_in,
    small_sem,
    load_sem,
    ready,
    sent_sem,
    pair_recv,
    code_recv,
    chip_recv,
    side_recv,
    fwd_recv,
    core_recv,
    red_recv,
    early_recv,
    late_recv,
    back_recv,
    feat_recv,
    sq_recv,
):
    me, tp = lax.axis_index("ep"), lax.axis_index("tp")
    core = lax.rem(me, 2)
    chip = lax.div(me, 2)
    odd = lax.rem(tp, 2)
    partner = me + 1 - 2 * core
    beside = {"tp": tp + 1 - 2 * odd}
    chips = ep_size // 2
    toks, width = tok_ref.shape
    experts, _, _, ff = gu_buf.shape
    out_width = width // tp_size
    cut = out_width // 2
    depth = width // PIECES
    direct = PIECES - SIDE

    def chip_at(step):
        return lax.rem(chip + step, chips)

    def tp_at(step):
        return lax.rem(tp + step, tp_size)

    def send(src, dst, send_sem, recv_sem, device):
        return pltpu.make_async_remote_copy(
            src_ref=src,
            dst_ref=dst,
            send_sem=send_sem,
            recv_sem=recv_sem,
            device_id=device,
            device_id_type=MESH,
        )

    sent = []

    def start(src, dst, recv_sem, device):
        copy = send(src, dst, sent_sem, recv_sem, device)
        copy.start()
        sent.append(copy)

    def arrived(slot, sem):
        send(slot, slot, sent_sem, sem, {"ep": partner}).wait_recv()

    def tell(sem):
        @pl.when(tp > 0)
        def _():
            pl.semaphore_signal(sem, inc=1, device_id={"tp": tp - 1}, device_id_type=MESH)

        @pl.when(tp < tp_size - 1)
        def _():
            pl.semaphore_signal(sem, inc=1, device_id={"tp": tp + 1}, device_id_type=MESH)

    def learn(r):
        pl.semaphore_wait(ready.at[r], beside_count)
        if r + 1 < tp_size - 2:
            tell(ready.at[r + 1])

    beside_count = lax.div(tp + tp_size - 1, tp_size) + lax.div(2 * tp_size - 2 - tp, tp_size)

    loads = []
    for e in range(experts):
        loads.append((gate_hbm.at[e], gu_buf.at[e, 0], e))
        loads.append((up_hbm.at[e], gu_buf.at[e, 1], e))
    for e in range(experts):
        loads.append((down_hbm.at[e], down_buf.at[pl.ds(e * ff, ff)], experts))
    loads = [pltpu.make_async_copy(src, dst, load_sem.at[i]) for src, dst, i in loads]

    def loaded(slot, i):
        pltpu.make_async_copy(slot, slot, load_sem.at[i]).wait()

    smalls = (
        (tok_hbm, tok_ref),
        (gain_hbm, gain_ref),
        (route_hbm, route_ref),
        (weight_hbm, weight_ref),
        (out_gain_hbm, out_gain_ref),
    )
    smalls = [
        pltpu.make_async_copy(src, dst, small_sem.at[i]) for i, (src, dst) in enumerate(smalls)
    ]
    barrier = pltpu.get_barrier_semaphore()
    for load in smalls:
        load.start()
    for step in range(1, ep_size):
        pl.semaphore_signal(
            barrier, inc=1, device_id={"ep": lax.rem(me + step, ep_size)}, device_id_type=MESH
        )
    tell(barrier)
    for load in loads:
        load.start()

    for load in smalls[:2]:
        load.wait()
    scaled = tok_ref[...].astype(F32)
    scale = lax.rsqrt(jnp.mean(scaled * scaled, axis=-1, keepdims=True) + EPS)
    scaled = (scaled * scale * gain_ref[...]).astype(BF16)
    for p in range(PIECES):
        rows[me, p] = scaled[:, p * depth : (p + 1) * depth]

    pl.semaphore_wait(barrier, ep_size - 1 + beside_count)

    def piece(slot, j):
        return rows.at[slot, j + odd * (PIECES - 1 - 2 * j)]

    for j in range(direct):
        for step in range(1, chips):
            block = piece(me, j)
            start(block, block, chip_recv.at[step - 1, j], {"ep": 2 * chip_at(step) + core})
        if j == 0:
            start(rows.at[me], rows.at[me], pair_recv, {"ep": partner})
    if tp_size > 2:
        tell(ready.at[0])

    for load in smalls[2:4]:
        load.wait()
    place = lax.broadcasted_iota(jnp.int32, (codes.shape[1], toks), 0)
    placed = jnp.zeros(place.shape, F32)
    for k in range(route_ref.shape[0]):
        placed = placed + jnp.where(place == route_ref[k : k + 1], weight_ref[k : k + 1], 0.0)
    codes[me] = jnp.zeros(codes.shape[1:], F32)
    codes[me, :, :toks] = placed
    start(codes.at[me], codes.at[me], code_recv.at[0], {"ep": partner})
    for step in range(1, chips):
        for other in range(2):
            start(
                codes.at[me],
                codes.at[me],
                code_recv.at[1],
                {"ep": 2 * chip_at(step) + other},
            )

    def mixes(index):
        columns = jnp.concatenate([codes[2 * index + c].T[:toks] for c in range(2)], axis=0)
        lane = lax.broadcasted_iota(jnp.int32, columns.shape, 1)
        return [
            jnp.sum(jnp.where(lane == me * experts + e, columns, 0.0), axis=1, keepdims=True)
            for e in range(experts)
        ]

    def features(index, first, count):
        both = pl.ds(2 * index, 2)
        parts = [rows[both, first + t].reshape(2 * toks, depth) for t in range(count)]
        return jnp.concatenate(parts, axis=1)

    def activate(index, e, gate, up, mix):
        gate = jnp.minimum(gate, LIMIT)
        up = jnp.clip(up, -LIMIT, LIMIT)
        act = (up + 1.0) * gate * jax.nn.sigmoid(ALPHA * gate) * mix
        act = act.astype(BF16).reshape(2, toks, ff)
        hidden[pl.ds(2 * index, 2), :, e * ff : (e + 1) * ff] = act

    def own_expert(e, mix):
        x = features(chip, 0, PIECES)
        loaded(gu_buf.at[e], e)
        gate = jnp.dot(x, gu_buf[e, 0], preferred_element_type=F32)
        up = jnp.dot(x, gu_buf[e, 1], preferred_element_type=F32)
        activate(chip, e, gate, up, mix)

    def other_experts(index, number, mix):
        a, b = CHUNKS[number]
        first = a + odd * (PIECES - a - b)
        x = features(index, first, b - a)
        part = pl.ds(pl.multiple_of(first * depth, depth), (b - a) * depth)
        for e in range(experts):
            sums = []
            for i in range(2):
                total = jnp.dot(x, gu_buf[e, i, part, :], preferred_element_type=F32)
                if number:
                    total = total + acc[e, i]
                sums.append(total)
            if number == len(CHUNKS) - 1:
                activate(index, e, sums[0], sums[1], mix[e])
            else:
                for i in range(2):
                    acc[e, i] = sums[i]

    def forward(j):
        number = [a <= j < b for a, b in CHUNKS].index(True)
        for step in range(1, chips):
            block = piece(2 * chip_at(chips - step) + core, j)
            if j < direct:
                arrived(block, chip_recv.at[step - 1, j])
            else:
                arrived(block, side_recv.at[step - 1, j - direct])
            if j < SIDE:
                start(block, block, side_recv.at[step - 1, SIDE - 1 - j], beside)
            start(block, block, fwd_recv.at[step - 1, number], {"ep": partner})

    order = [0] * (tp_size - 1)
    for t in range(tp_size):
        here = 1 - lax.div((tp - t) * (tp - t) + tp_size * tp_size - 1, tp_size * tp_size)
        far = sorted((o for o in range(tp_size) if o != t), key=lambda o: -abs(o - t))
        order = [k + here * ((o - t) % tp_size) for k, o in zip(order, far)]
    order.append(0)

    def own(k):
        return isinstance(k, int)

    def project(step, k):
        index = chip_at(step)
        both = jnp.concatenate([hidden[2 * index + 1 - core], hidden[2 * index + core]], axis=0)
        columns = pl.ds(pl.multiple_of(tp_at(k) * out_width, out_width), out_width)
        out = jnp.dot(both, down_buf[:, columns], preferred_element_type=F32)
        core_out[step, k] = out[:toks].astype(BF16)
        core_sum[step, k] = out[toks:]
        start(
            core_out.at[step, k], core_in.at[step, k], core_recv.at[step, k], {"ep": partner}
        )

    def crossed(step, k):
        block = core_in.at[step, k]
        arrived(block, core_recv.at[step, k])
        return core_sum[step, k] + block[...].astype(F32)

    def own_chip(k):
        total = crossed(0, k)
        own_sum[k] = total[:, :cut]
        if not own(k):
            early_out[k - 1] = total[:, cut:].astype(BF16)
            start(early_out.at[k - 1], early_in.at[k - 1], early_recv, {"tp": tp_at(k)})
        else:
            near_sum[...] = total[:, cut:]

    def other_chip(step, k):
        total = crossed(step, k)
        slot = step - 1
        chip_out[k, slot] = total[:, :cut].astype(BF16)
        start(
            chip_out.at[k, slot],
            chip_in.at[k, slot],
            red_recv.at[k, slot],
            {"ep": 2 * chip_at(step) + core},
        )
        if not own(k):
            late_out[slot, k - 1] = total[:, cut:].astype(BF16)
            start(
                late_out.at[slot, k - 1],
                late_in.at[slot, k - 1],
                late_recv.at[slot],
                {"tp": tp_at(k)},
            )
        else:
            late_sum[slot] = total[:, cut:]

    arrived(rows.at[partner], pair_recv)
    arrived(codes.at[partner], code_recv.at[0])
    mix = mixes(chip)
    for e in range(experts):
        own_expert(e, mix[e])
    if tp_size > 2:
        learn(0)
    forward(0)
    loaded(down_buf, experts)
    for i, k in enumerate(order):
        project(0, k)
        if i == len(order) // 2 - 1:
            forward(1)
    forward(2)
    forward(3)
    for r in range(1, tp_size - 2):
        learn(r)
    for k in order:
        own_chip(k)
    for j in range(4, direct):
        forward(j)
    if chips > 1:
        arrived(codes.at[pl.ds(0, ep_size - 2)], code_recv.at[1])

    def sides():
        for j in range(PIECES - 1, direct - 1, -1):
            forward(j)

    sides()

    marked = len(sent)
    for step in range(1, chips):
        index = chip_at(chips - step)
        for number, (a, b) in enumerate(CHUNKS):
            first = a + odd * (PIECES - a - b)
            block = rows.at[2 * index + 1 - core, pl.ds(first, b - a)]
            arrived(block, fwd_recv.at[step - 1, number])
            if number == 0:
                mix = mixes(index)
            other_experts(index, number, mix)
            if number == 0 and step == 1:

                del sent[marked:]

        for k in order:
            project(chips - step, k)
        for k in order:
            other_chip(chips - step, k)

    for k in order:
        total = own_sum[k]
        for slot in range(chips - 1):
            block = chip_in.at[k, slot]
            arrived(block, red_recv.at[k, slot])
            total = total + block[...].astype(F32)
        if not own(k):
            feat_out[k - 1] = total.astype(BF16)
            start(feat_out.at[k - 1], feat_in.at[k - 1], feat_recv, {"tp": tp_at(k)})
        else:
            left = total
    for slot in range(chips - 1):
        total = late_sum[slot]
        arrived(late_in.at[slot], late_recv.at[slot])
        for k in range(1, tp_size):
            total = total + late_in[slot, k - 1].astype(F32)
        back_out[slot] = total.astype(BF16)
        start(
            back_out.at[slot],
            back_in.at[slot],
            back_recv,
            {"ep": 2 * chip_at(slot + 1) + core},
        )
    right = near_sum[...]
    arrived(early_in, early_recv)
    for k in range(1, tp_size):
        right = right + early_in[k - 1].astype(F32)
    arrived(feat_in, feat_recv)
    for k in range(1, tp_size):
        left = left + feat_in[k - 1].astype(F32)
    if chips > 1:
        arrived(back_in, back_recv)
    for slot in range(chips - 1):
        right = right + back_in[slot].astype(F32)
    mixed = jnp.concatenate([left, right], axis=1)

    squares = mixed * mixed
    folded = jnp.zeros((toks, LANES), F32)
    for j in range(out_width // LANES):
        folded = folded + squares[:, j * LANES : (j + 1) * LANES]
    wide = square_out.shape[1]
    if wide > toks:
        folded = jnp.concatenate([folded, jnp.zeros((wide - toks, LANES), F32)], axis=0)
    line = jnp.sum(folded.T, axis=0, keepdims=True)
    square_out[...] = jnp.broadcast_to(line, square_out.shape)
    for k in range(1, tp_size):
        start(square_out, square_in.at[k - 1], sq_recv, {"tp": tp_at(k)})
    arrived(square_in, sq_recv)
    for k in range(1, tp_size):
        line = line + square_in[k - 1, 0:1, :]
    total = jnp.broadcast_to(line, (LANES, wide)).T[:toks, :1]
    factor = lax.rsqrt(total / width + EPS)
    smalls[4].wait()
    out_ref[...] = (mixed * factor * out_gain_ref[...]).astype(BF16)
    for copy in sent:
        copy.wait_send()


def on_device(
    tokens, routing, route_weight, norm_gain, gate_weight, up_weight, down_weight, out_gain
):
    toks, width = tokens.shape
    experts, _, ff = gate_weight.shape
    ep_size, tp_size = lax.axis_size("ep"), lax.axis_size("tp")
    chips = ep_size // 2
    wide = pl.cdiv(toks, LANES) * LANES
    out_width = width // tp_size
    cut = out_width // 2
    vmem = pl.BlockSpec(memory_space=pltpu.VMEM)
    hbm = pl.BlockSpec(memory_space=pl.ANY)
    dma = pltpu.SemaphoreType.DMA
    return pl.pallas_call(
        functools.partial(kernel, ep_size, tp_size),
        out_shape=pltpu.VMEM((toks, out_width), BF16),
        in_specs=[hbm] * 8,
        out_specs=vmem,
        scratch_shapes=[
            pltpu.VMEM(tokens.shape, tokens.dtype),
            pltpu.VMEM(routing.shape[::-1], routing.dtype),
            pltpu.VMEM(routing.shape[::-1], F32),
            pltpu.VMEM((1, width), F32),
            pltpu.VMEM((1, out_width), F32),
            pltpu.VMEM((ep_size, PIECES, toks, width // PIECES), BF16),
            pltpu.VMEM((ep_size, pl.cdiv(experts * ep_size, 8) * 8, wide), F32),
            pltpu.VMEM((experts, 2, width, ff), BF16),
            pltpu.VMEM((experts * ff, width), BF16),
            pltpu.VMEM((experts, 2, 2 * toks, ff), F32),
            pltpu.VMEM((ep_size, toks, experts * ff), BF16),
            pltpu.VMEM((chips, tp_size, toks, out_width), BF16),
            pltpu.VMEM((chips, tp_size, toks, out_width), BF16),
            pltpu.VMEM((chips, tp_size, toks, out_width), F32),
            pltpu.VMEM((tp_size, toks, cut), F32),
            pltpu.VMEM((toks, cut), F32),
            pltpu.VMEM((chips - 1, toks, cut), F32),
            pltpu.VMEM((tp_size, chips - 1, toks, cut), BF16),
            pltpu.VMEM((tp_size, chips - 1, toks, cut), BF16),
            pltpu.VMEM((tp_size - 1, toks, cut), BF16),
            pltpu.VMEM((tp_size - 1, toks, cut), BF16),
            pltpu.VMEM((chips - 1, tp_size - 1, toks, cut), BF16),
            pltpu.VMEM((chips - 1, tp_size - 1, toks, cut), BF16),
            pltpu.VMEM((chips - 1, toks, cut), BF16),
            pltpu.VMEM((chips - 1, toks, cut), BF16),
            pltpu.VMEM((tp_size - 1, toks, cut), BF16),
            pltpu.VMEM((tp_size - 1, toks, cut), BF16),
            pltpu.VMEM((8, wide), F32),
            pltpu.VMEM((tp_size - 1, 8, wide), F32),
            dma((5,)),
            dma((experts + 1,)),
            pltpu.SemaphoreType.REGULAR((tp_size - 2,)),
            dma,
            dma,
            dma((2,)),
            dma((chips - 1, PIECES - SIDE)),
            dma((chips - 1, SIDE)),
            dma((chips - 1, len(CHUNKS))),
            dma((chips, tp_size)),
            dma((tp_size, chips - 1)),
            dma,
            dma((chips - 1,)),
            dma,
            dma,
            dma,
        ],
        compiler_params=pltpu.CompilerParams(
            collective_id=0, has_side_effects=True, vmem_limit_bytes=60 * 1024 * 1024
        ),
    )(
        tokens,
        routing.T,
        route_weight.T,
        norm_gain.reshape(1, width),
        out_gain.reshape(1, out_width),
        gate_weight,
        up_weight,
        down_weight,
    )


def solution(mesh):
    in_specs = (
        P(("grp", "ep"), None),
        P(("grp", "ep"), None),
        P(("grp", "ep"), None),
        P(),
        P("ep", None, "tp"),
        P("ep", None, "tp"),
        P("ep", "tp", None),
        P("tp"),
    )
    out_specs = P(("grp", "ep"), "tp")
    return jax.shard_map(
        on_device, mesh=mesh, in_specs=in_specs, out_specs=out_specs, check_vma=False
    )
```

```python
import functools

import jax
import jax.numpy as jnp
from jax import lax
from jax.experimental import pallas as pl
from jax.experimental.pallas import tpu as pltpu
from jax.sharding import PartitionSpec as P

LIMIT = 7.0
ALPHA = 1.702
EPS = 1e-06
LANES = 128
PIECES = 16
SIDE = 4
CHUNKS = ((0, 8), (8, 12), (12, 16))
MESH = pl.DeviceIdType.MESH
BF16 = jnp.bfloat16
F32 = jnp.float32


def kernel(
    ep_size,
    tp_size,
    tok_hbm,
    route_hbm,
    weight_hbm,
    gain_hbm,
    out_gain_hbm,
    gate_hbm,
    up_hbm,
    down_hbm,
    out_ref,
    tok_ref,
    route_ref,
    weight_ref,
    gain_ref,
    out_gain_ref,
    rows,
    codes,
    gu_buf,
    down_buf,
    acc,
    hidden,
    core_out,
    core_in,
    core_sum,
    own_sum,
    near_sum,
    late_sum,
    chip_out,
    chip_in,
    early_out,
    early_in,
    late_out,
    late_in,
    back_out,
    back_in,
    feat_out,
    feat_in,
    square_out,
    square_in,
    small_sem,
    load_sem,
    ready,
    turn,
    sent_sem,
    pair_recv,
    code_recv,
    chip_recv,
    side_recv,
    fwd_recv,
    core_recv,
    red_recv,
    early_recv,
    late_recv,
    back_recv,
    feat_recv,
    sq_recv,
):
    me, tp = lax.axis_index("ep"), lax.axis_index("tp")
    core = lax.rem(me, 2)
    chip = lax.div(me, 2)
    odd = lax.rem(tp, 2)
    partner = me + 1 - 2 * core
    beside = {"tp": tp + 1 - 2 * odd}
    chips = ep_size // 2
    toks, width = tok_ref.shape
    experts, _, _, ff = gu_buf.shape
    out_width = width // tp_size
    cut = out_width // 2
    depth = width // PIECES
    direct = PIECES - SIDE

    chip_table = [lax.rem(chip + step, chips) for step in range(chips)]

    def chip_at(step):
        return chip_table[step]

    def tp_at(step):
        return lax.rem(tp + step, tp_size)

    def send(src, dst, send_sem, recv_sem, device):
        return pltpu.make_async_remote_copy(
            src_ref=src,
            dst_ref=dst,
            send_sem=send_sem,
            recv_sem=recv_sem,
            device_id=device,
            device_id_type=MESH,
        )

    sent = []

    def start(src, dst, recv_sem, device):
        copy = send(src, dst, sent_sem, recv_sem, device)
        copy.start()
        sent.append(src)

    def arrived(slot, sem):
        send(slot, slot, sent_sem, sem, {"ep": partner}).wait_recv()

    def tell(sem):
        @pl.when(tp > 0)
        def _():
            pl.semaphore_signal(sem, inc=1, device_id={"tp": tp - 1}, device_id_type=MESH)

        @pl.when(tp < tp_size - 1)
        def _():
            pl.semaphore_signal(sem, inc=1, device_id={"tp": tp + 1}, device_id_type=MESH)

    def learn(r):
        pl.semaphore_wait(ready.at[r], beside_count)
        if r + 1 < tp_size - 2:
            tell(ready.at[r + 1])

    beside_count = lax.div(tp + tp_size - 1, tp_size) + lax.div(2 * tp_size - 2 - tp, tp_size)

    loads = []
    for e in range(experts):
        loads.append((gate_hbm.at[e], gu_buf.at[e, 0], e))
        loads.append((up_hbm.at[e], gu_buf.at[e, 1], e))
    for e in range(experts):
        loads.append((down_hbm.at[e], down_buf.at[pl.ds(e * ff, ff)], experts))
    loads = [pltpu.make_async_copy(src, dst, load_sem.at[i]) for src, dst, i in loads]

    def loaded(slot, i):
        pltpu.make_async_copy(slot, slot, load_sem.at[i]).wait()

    smalls = (
        (tok_hbm, tok_ref),
        (gain_hbm, gain_ref),
        (route_hbm, route_ref),
        (weight_hbm, weight_ref),
        (out_gain_hbm, out_gain_ref),
    )
    smalls = [
        pltpu.make_async_copy(src, dst, small_sem.at[i]) for i, (src, dst) in enumerate(smalls)
    ]
    barrier = pltpu.get_barrier_semaphore()
    for load in smalls:
        load.start()
    for step in range(1, ep_size):
        pl.semaphore_signal(
            barrier, inc=1, device_id={"ep": lax.rem(me + step, ep_size)}, device_id_type=MESH
        )
    tell(barrier)
    for load in loads:
        load.start()

    for load in smalls[:2]:
        load.wait()
    scaled = tok_ref[...].astype(F32)
    scale = lax.rsqrt(jnp.mean(scaled * scaled, axis=-1, keepdims=True) + EPS)
    scaled = (scaled * scale * gain_ref[...]).astype(BF16)
    for p in range(PIECES):
        rows[me, p] = scaled[:, p * depth : (p + 1) * depth]

    pl.semaphore_wait(barrier, ep_size - 1 + beside_count)

    def piece(slot, j):
        return rows.at[slot, j + odd * (PIECES - 1 - 2 * j)]

    def send_pieces():
        for j in range(direct):
            for step in range(1, chips):
                block = piece(me, j)
                slot = chip_recv.at[step - 1, j]
                start(block, block, slot, {"ep": 2 * chip_at(step) + core})

    start(rows.at[me], rows.at[me], pair_recv, {"ep": partner})

    send_pieces()
    if tp_size > 2:
        tell(ready.at[0])

    for load in smalls[2:4]:
        load.wait()
    place = lax.broadcasted_iota(jnp.int32, (codes.shape[1], toks), 0)
    placed = jnp.zeros(place.shape, F32)
    for k in range(route_ref.shape[0]):
        placed = placed + jnp.where(place == route_ref[k : k + 1], weight_ref[k : k + 1], 0.0)
    codes[me] = jnp.zeros(codes.shape[1:], F32)
    codes[me, :, :toks] = placed
    start(codes.at[me], codes.at[me], code_recv.at[0], {"ep": partner})
    for step in range(1, chips):
        for other in range(2):
            start(
                codes.at[me],
                codes.at[me],
                code_recv.at[1],
                {"ep": 2 * chip_at(step) + other},
            )

    def mixes(index):
        columns = jnp.concatenate([codes[2 * index + c].T[:toks] for c in range(2)], axis=0)
        lane = lax.broadcasted_iota(jnp.int32, columns.shape, 1)
        return [
            jnp.sum(jnp.where(lane == me * experts + e, columns, 0.0), axis=1, keepdims=True)
            for e in range(experts)
        ]

    def features(index, first, count):
        both = pl.ds(2 * index, 2)
        parts = [rows[both, first + t].reshape(2 * toks, depth) for t in range(count)]
        return jnp.concatenate(parts, axis=1)

    def activate(index, e, gate, up, mix):
        gate = jnp.minimum(gate, LIMIT)
        up = jnp.clip(up, -LIMIT, LIMIT)
        act = (up + 1.0) * gate * jax.nn.sigmoid(ALPHA * gate) * mix
        act = act.astype(BF16).reshape(2, toks, ff)
        hidden[pl.ds(2 * index, 2), :, e * ff : (e + 1) * ff] = act

    def own_expert(e, mix):
        x = features(chip, 0, PIECES)
        loaded(gu_buf.at[e], e)
        gate = jnp.dot(x, gu_buf[e, 0], preferred_element_type=F32)
        up = jnp.dot(x, gu_buf[e, 1], preferred_element_type=F32)
        activate(chip, e, gate, up, mix)

    def other_experts(index, number, mix):
        a, b = CHUNKS[number]
        first = a + odd * (PIECES - a - b)
        x = features(index, first, b - a)
        part = pl.ds(pl.multiple_of(first * depth, depth), (b - a) * depth)
        for e in range(experts):
            sums = []
            for i in range(2):
                total = jnp.dot(x, gu_buf[e, i, part, :], preferred_element_type=F32)
                if number:
                    total = total + acc[e, i]
                sums.append(total)
            if number == len(CHUNKS) - 1:
                activate(index, e, sums[0], sums[1], mix[e])
            else:
                for i in range(2):
                    acc[e, i] = sums[i]

    def forward(j):
        number = [a <= j < b for a, b in CHUNKS].index(True)
        for step in range(1, chips):
            block = piece(2 * chip_at(chips - step) + core, j)
            if j < direct:
                arrived(block, chip_recv.at[step - 1, j])
            else:
                arrived(block, side_recv.at[step - 1, j - direct])
            if j < SIDE:
                start(block, block, side_recv.at[step - 1, SIDE - 1 - j], beside)
            start(block, block, fwd_recv.at[step - 1, number], {"ep": partner})

    order = [0] * (tp_size - 1)
    for t in range(tp_size):
        here = 1 - lax.div((tp - t) * (tp - t) + tp_size * tp_size - 1, tp_size * tp_size)
        far = sorted((o for o in range(tp_size) if o != t), key=lambda o: -abs(o - t))
        order = [k + here * ((o - t) % tp_size) for k, o in zip(order, far)]
    order.append(0)

    def own(k):
        return isinstance(k, int)

    def project(step, k):
        index = chip_at(step)
        both = jnp.concatenate([hidden[2 * index + 1 - core], hidden[2 * index + core]], axis=0)
        columns = pl.ds(pl.multiple_of(tp_at(k) * out_width, out_width), out_width)
        out = jnp.dot(both, down_buf[:, columns], preferred_element_type=F32)
        core_out[step, k] = out[:toks].astype(BF16)
        core_sum[step, k] = out[toks:]
        start(
            core_out.at[step, k], core_in.at[step, k], core_recv.at[step, k], {"ep": partner}
        )

    def crossed(step, k):
        block = core_in.at[step, k]
        arrived(block, core_recv.at[step, k])
        return core_sum[step, k] + block[...].astype(F32)

    def own_chip(k):
        total = crossed(0, k)
        own_sum[k] = total[:, :cut]
        if not own(k):
            early_out[k - 1] = total[:, cut:].astype(BF16)
            start(early_out.at[k - 1], early_in.at[k - 1], early_recv, {"tp": tp_at(k)})
        else:
            near_sum[...] = total[:, cut:]

    def other_chip(step, k):
        total = crossed(step, k)
        slot = step - 1
        chip_out[k, slot] = total[:, :cut].astype(BF16)
        start(
            chip_out.at[k, slot],
            chip_in.at[k, slot],
            red_recv.at[k, slot],
            {"ep": 2 * chip_at(step) + core},
        )
        if not own(k):
            late_out[slot, k - 1] = total[:, cut:].astype(BF16)
            start(
                late_out.at[slot, k - 1],
                late_in.at[slot, k - 1],
                late_recv.at[slot],
                {"tp": tp_at(k)},
            )
        else:
            late_sum[slot] = total[:, cut:]

    arrived(rows.at[partner], pair_recv)
    arrived(codes.at[partner], code_recv.at[0])
    mix = mixes(chip)
    for e in range(experts):
        own_expert(e, mix[e])
    forward(0)
    forward(1)
    if tp_size > 2:
        learn(0)
    loaded(down_buf, experts)
    for i, k in enumerate(order):
        project(0, k)
        if i == len(order) // 4 - 1:
            forward(2)
            forward(3)
        if i == 3 * len(order) // 4 - 1:
            forward(4)
            forward(5)
    forward(6)
    forward(7)
    for r in range(1, tp_size - 2):
        learn(r)
    for k in order:
        own_chip(k)
    for j in range(8, direct):
        forward(j)
    if chips > 1:
        arrived(codes.at[pl.ds(0, ep_size - 2)], code_recv.at[1])

    def sides():
        for j in range(PIECES - 1, direct - 1, -1):
            forward(j)

    marked = len(sent)

    @pl.when(core == 1)
    def _():
        sides()

    for step in range(1, chips):
        index = chip_at(chips - step)
        for number, (a, b) in enumerate(CHUNKS):
            first = a + odd * (PIECES - a - b)
            block = rows.at[2 * index + 1 - core, pl.ds(first, b - a)]
            arrived(block, fwd_recv.at[step - 1, number])
            if number == 0:
                mix = mixes(index)
            other_experts(index, number, mix)
            if number == 0 and step == 1:

                @pl.when(core == 0)
                def _():
                    sides()

                del sent[marked:]
                sent.extend([rows.at[me, 0]] * (SIDE * (chips - 1)))

        for k in order:
            project(chips - step, k)

        @pl.when(core == 1)
        def _():
            pl.semaphore_wait(turn, 1)

        for k in order:
            other_chip(chips - step, k)

        @pl.when(core == 0)
        def _():
            pl.semaphore_signal(turn, inc=1, device_id={"ep": partner}, device_id_type=MESH)

    def reduced(k):
        total = own_sum[k]
        for slot in range(chips - 1):
            block = chip_in.at[k, slot]
            arrived(block, red_recv.at[k, slot])
            total = total + block[...].astype(F32)
        return total

    def own_features(k):
        feat_out[k - 1] = reduced(k).astype(BF16)
        start(feat_out.at[k - 1], feat_in.at[k - 1], feat_recv, {"tp": tp_at(k)})

    for k in order[:-2]:
        own_features(k)
    for slot in range(chips - 1):
        total = late_sum[slot]
        arrived(late_in.at[slot], late_recv.at[slot])
        for k in range(1, tp_size):
            total = total + late_in[slot, k - 1].astype(F32)
        back_out[slot] = total.astype(BF16)
        start(
            back_out.at[slot],
            back_in.at[slot],
            back_recv,
            {"ep": 2 * chip_at(slot + 1) + core},
        )
    own_features(order[-2])
    left = reduced(0)
    right = near_sum[...]
    arrived(early_in, early_recv)
    for k in range(1, tp_size):
        right = right + early_in[k - 1].astype(F32)
    arrived(feat_in, feat_recv)
    for k in range(1, tp_size):
        left = left + feat_in[k - 1].astype(F32)
    if chips > 1:
        arrived(back_in, back_recv)
    for slot in range(chips - 1):
        right = right + back_in[slot].astype(F32)
    mixed = jnp.concatenate([left, right], axis=1)

    squares = mixed * mixed
    folded = jnp.zeros((toks, LANES), F32)
    for j in range(out_width // LANES):
        folded = folded + squares[:, j * LANES : (j + 1) * LANES]
    wide = square_out.shape[1]
    if wide > toks:
        folded = jnp.concatenate([folded, jnp.zeros((wide - toks, LANES), F32)], axis=0)
    line = jnp.sum(folded.T, axis=0, keepdims=True)
    square_out[...] = jnp.broadcast_to(line, square_out.shape)
    for k in range(1, tp_size):
        start(square_out, square_in.at[k - 1], sq_recv, {"tp": tp_at(k)})
    arrived(square_in, sq_recv)
    for k in range(1, tp_size):
        line = line + square_in[k - 1, 0:1, :]
    total = jnp.broadcast_to(line, (LANES, wide)).T[:toks, :1]
    factor = lax.rsqrt(total / width + EPS)
    smalls[4].wait()
    out_ref[...] = (mixed * factor * out_gain_ref[...]).astype(BF16)
    for src in sent:
        send(src, src, sent_sem, sent_sem, {"ep": partner}).wait_send()


def on_device(
    tokens, routing, route_weight, norm_gain, gate_weight, up_weight, down_weight, out_gain
):
    toks, width = tokens.shape
    experts, _, ff = gate_weight.shape
    ep_size, tp_size = lax.axis_size("ep"), lax.axis_size("tp")
    chips = ep_size // 2
    wide = pl.cdiv(toks, LANES) * LANES
    out_width = width // tp_size
    cut = out_width // 2
    vmem = pl.BlockSpec(memory_space=pltpu.VMEM)
    hbm = pl.BlockSpec(memory_space=pl.ANY)
    dma = pltpu.SemaphoreType.DMA
    return pl.pallas_call(
        functools.partial(kernel, ep_size, tp_size),
        out_shape=pltpu.VMEM((toks, out_width), BF16),
        in_specs=[hbm] * 8,
        out_specs=vmem,
        scratch_shapes=[
            pltpu.VMEM(tokens.shape, tokens.dtype),
            pltpu.VMEM(routing.shape[::-1], routing.dtype),
            pltpu.VMEM(routing.shape[::-1], F32),
            pltpu.VMEM((1, width), F32),
            pltpu.VMEM((1, out_width), F32),
            pltpu.VMEM((ep_size, PIECES, toks, width // PIECES), BF16),
            pltpu.VMEM((ep_size, pl.cdiv(experts * ep_size, 8) * 8, wide), F32),
            pltpu.VMEM((experts, 2, width, ff), BF16),
            pltpu.VMEM((experts * ff, width), BF16),
            pltpu.VMEM((experts, 2, 2 * toks, ff), F32),
            pltpu.VMEM((ep_size, toks, experts * ff), BF16),
            pltpu.VMEM((chips, tp_size, toks, out_width), BF16),
            pltpu.VMEM((chips, tp_size, toks, out_width), BF16),
            pltpu.VMEM((chips, tp_size, toks, out_width), F32),
            pltpu.VMEM((tp_size, toks, cut), F32),
            pltpu.VMEM((toks, cut), F32),
            pltpu.VMEM((chips - 1, toks, cut), F32),
            pltpu.VMEM((tp_size, chips - 1, toks, cut), BF16),
            pltpu.VMEM((tp_size, chips - 1, toks, cut), BF16),
            pltpu.VMEM((tp_size - 1, toks, cut), BF16),
            pltpu.VMEM((tp_size - 1, toks, cut), BF16),
            pltpu.VMEM((chips - 1, tp_size - 1, toks, cut), BF16),
            pltpu.VMEM((chips - 1, tp_size - 1, toks, cut), BF16),
            pltpu.VMEM((chips - 1, toks, cut), BF16),
            pltpu.VMEM((chips - 1, toks, cut), BF16),
            pltpu.VMEM((tp_size - 1, toks, cut), BF16),
            pltpu.VMEM((tp_size - 1, toks, cut), BF16),
            pltpu.VMEM((8, wide), F32),
            pltpu.VMEM((tp_size - 1, 8, wide), F32),
            dma((5,)),
            dma((experts + 1,)),
            pltpu.SemaphoreType.REGULAR((tp_size - 2,)),
            pltpu.SemaphoreType.REGULAR,
            dma,
            dma,
            dma((2,)),
            dma((chips - 1, PIECES - SIDE)),
            dma((chips - 1, SIDE)),
            dma((chips - 1, len(CHUNKS))),
            dma((chips, tp_size)),
            dma((tp_size, chips - 1)),
            dma,
            dma((chips - 1,)),
            dma,
            dma,
            dma,
        ],
        compiler_params=pltpu.CompilerParams(
            collective_id=0, has_side_effects=True, vmem_limit_bytes=60 * 1024 * 1024
        ),
    )(
        tokens,
        routing.T,
        route_weight.T,
        norm_gain.reshape(1, width),
        out_gain.reshape(1, out_width),
        gate_weight,
        up_weight,
        down_weight,
    )


def solution(mesh):
    in_specs = (
        P(("grp", "ep"), None),
        P(("grp", "ep"), None),
        P(("grp", "ep"), None),
        P(),
        P("ep", None, "tp"),
        P("ep", None, "tp"),
        P("ep", "tp", None),
        P("tp"),
    )
    out_specs = P(("grp", "ep"), "tp")
    return jax.shard_map(
        on_device, mesh=mesh, in_specs=in_specs, out_specs=out_specs, check_vma=False
    )
```

```python
import functools

import jax
import jax.numpy as jnp
from jax import lax
from jax.experimental import pallas as pl
from jax.experimental.pallas import tpu as pltpu
from jax.sharding import PartitionSpec as P

LIMIT = 7.0
ALPHA = 1.702
EPS = 1e-06
LANES = 128
PIECES = 16
SIDE = 4
CHUNKS = ((0, 8), (8, 12), (12, 16))
MESH = pl.DeviceIdType.MESH
BF16 = jnp.bfloat16
F32 = jnp.float32


def kernel(
    ep_size,
    tp_size,
    tok_hbm,
    route_hbm,
    weight_hbm,
    gain_hbm,
    out_gain_hbm,
    gate_hbm,
    up_hbm,
    down_hbm,
    out_ref,
    tok_ref,
    route_ref,
    weight_ref,
    gain_ref,
    out_gain_ref,
    rows,
    codes,
    gu_buf,
    down_buf,
    acc,
    hidden,
    core_out,
    core_in,
    core_sum,
    own_sum,
    near_sum,
    late_sum,
    chip_out,
    chip_in,
    early_out,
    early_in,
    late_out,
    late_in,
    back_out,
    back_in,
    feat_out,
    feat_in,
    square_out,
    square_in,
    small_sem,
    load_sem,
    ready,
    turn,
    sent_sem,
    chip_sem,
    pair_recv,
    code_recv,
    chip_recv,
    side_recv,
    fwd_recv,
    core_recv,
    red_recv,
    early_recv,
    late_recv,
    back_recv,
    feat_recv,
    sq_recv,
):
    me, tp = lax.axis_index("ep"), lax.axis_index("tp")
    core = lax.rem(me, 2)
    chip = lax.div(me, 2)
    odd = lax.rem(tp, 2)
    partner = me + 1 - 2 * core
    beside = {"tp": tp + 1 - 2 * odd}
    chips = ep_size // 2
    toks, width = tok_ref.shape
    experts, _, _, ff = gu_buf.shape
    out_width = width // tp_size
    cut = out_width // 2
    depth = width // PIECES
    direct = PIECES - SIDE

    chip_table = [lax.rem(chip + step, chips) for step in range(chips)]

    def chip_at(step):
        return chip_table[step]

    def tp_at(step):
        return lax.rem(tp + step, tp_size)

    def send(src, dst, send_sem, recv_sem, device):
        return pltpu.make_async_remote_copy(
            src_ref=src,
            dst_ref=dst,
            send_sem=send_sem,
            recv_sem=recv_sem,
            device_id=device,
            device_id_type=MESH,
        )

    sent = []

    def start(src, dst, recv_sem, device, out_sem=sent_sem):
        copy = send(src, dst, out_sem, recv_sem, device)
        copy.start()
        if out_sem is sent_sem:
            sent.append(src)

    def arrived(slot, sem):
        send(slot, slot, sent_sem, sem, {"ep": partner}).wait_recv()

    def tell(sem):
        @pl.when(tp > 0)
        def _():
            pl.semaphore_signal(sem, inc=1, device_id={"tp": tp - 1}, device_id_type=MESH)

        @pl.when(tp < tp_size - 1)
        def _():
            pl.semaphore_signal(sem, inc=1, device_id={"tp": tp + 1}, device_id_type=MESH)

    def learn(r):
        pl.semaphore_wait(ready.at[r], beside_count)
        if r + 1 < tp_size - 2:
            tell(ready.at[r + 1])

    beside_count = lax.div(tp + tp_size - 1, tp_size) + lax.div(2 * tp_size - 2 - tp, tp_size)

    loads = []
    for e in range(experts):
        loads.append((gate_hbm.at[e], gu_buf.at[e, 0], e))
        loads.append((up_hbm.at[e], gu_buf.at[e, 1], e))
    for e in range(experts):
        loads.append((down_hbm.at[e], down_buf.at[pl.ds(e * ff, ff)], experts))
    loads = [pltpu.make_async_copy(src, dst, load_sem.at[i]) for src, dst, i in loads]

    def loaded(slot, i):
        pltpu.make_async_copy(slot, slot, load_sem.at[i]).wait()

    smalls = (
        (tok_hbm, tok_ref),
        (gain_hbm, gain_ref),
        (route_hbm, route_ref),
        (weight_hbm, weight_ref),
        (out_gain_hbm, out_gain_ref),
    )
    smalls = [
        pltpu.make_async_copy(src, dst, small_sem.at[i]) for i, (src, dst) in enumerate(smalls)
    ]
    barrier = pltpu.get_barrier_semaphore()
    for load in smalls:
        load.start()
    for step in range(1, ep_size):
        pl.semaphore_signal(
            barrier, inc=1, device_id={"ep": lax.rem(me + step, ep_size)}, device_id_type=MESH
        )
    tell(barrier)
    for load in loads:
        load.start()

    for load in smalls[:2]:
        load.wait()
    scaled = tok_ref[...].astype(F32)
    scale = lax.rsqrt(jnp.mean(scaled * scaled, axis=-1, keepdims=True) + EPS)
    scaled = (scaled * scale * gain_ref[...]).astype(BF16)
    for p in range(PIECES):
        rows[me, p] = scaled[:, p * depth : (p + 1) * depth]

    pl.semaphore_wait(barrier, ep_size - 1 + beside_count)

    def piece(slot, j):
        return rows.at[slot, j + odd * (PIECES - 1 - 2 * j)]

    def send_pieces():
        for j in range(direct):
            for step in range(1, chips):
                block = piece(me, j)
                slot = chip_recv.at[step - 1, j]
                start(block, block, slot, {"ep": 2 * chip_at(step) + core})

    start(rows.at[me], rows.at[me], pair_recv, {"ep": partner})

    send_pieces()
    if tp_size > 2:
        tell(ready.at[0])

    for load in smalls[2:4]:
        load.wait()
    place = lax.broadcasted_iota(jnp.int32, (codes.shape[1], toks), 0)
    placed = jnp.zeros(place.shape, F32)
    for k in range(route_ref.shape[0]):
        placed = placed + jnp.where(place == route_ref[k : k + 1], weight_ref[k : k + 1], 0.0)
    codes[me] = jnp.zeros(codes.shape[1:], F32)
    codes[me, :, :toks] = placed
    start(codes.at[me], codes.at[me], code_recv.at[0], {"ep": partner})
    for step in range(1, chips):
        for other in range(2):
            start(
                codes.at[me],
                codes.at[me],
                code_recv.at[1],
                {"ep": 2 * chip_at(step) + other},
            )

    def mixes(index):
        columns = jnp.concatenate([codes[2 * index + c].T[:toks] for c in range(2)], axis=0)
        lane = lax.broadcasted_iota(jnp.int32, columns.shape, 1)
        return [
            jnp.sum(jnp.where(lane == me * experts + e, columns, 0.0), axis=1, keepdims=True)
            for e in range(experts)
        ]

    def features(index, first, count):
        both = pl.ds(2 * index, 2)
        parts = [rows[both, first + t].reshape(2 * toks, depth) for t in range(count)]
        return jnp.concatenate(parts, axis=1)

    def activate(index, e, gate, up, mix):
        gate = jnp.minimum(gate, LIMIT)
        up = jnp.clip(up, -LIMIT, LIMIT)
        act = (up + 1.0) * gate * jax.nn.sigmoid(ALPHA * gate) * mix
        act = act.astype(BF16).reshape(2, toks, ff)
        hidden[pl.ds(2 * index, 2), :, e * ff : (e + 1) * ff] = act

    def own_expert(e, mix):
        x = features(chip, 0, PIECES)
        loaded(gu_buf.at[e], e)
        gate = jnp.dot(x, gu_buf[e, 0], preferred_element_type=F32)
        up = jnp.dot(x, gu_buf[e, 1], preferred_element_type=F32)
        activate(chip, e, gate, up, mix)

    def other_experts(index, number, mix):
        a, b = CHUNKS[number]
        first = a + odd * (PIECES - a - b)
        x = features(index, first, b - a)
        part = pl.ds(pl.multiple_of(first * depth, depth), (b - a) * depth)
        for e in range(experts):
            sums = []
            for i in range(2):
                total = jnp.dot(x, gu_buf[e, i, part, :], preferred_element_type=F32)
                if number:
                    total = total + acc[e, i]
                sums.append(total)
            if number == len(CHUNKS) - 1:
                activate(index, e, sums[0], sums[1], mix[e])
            else:
                for i in range(2):
                    acc[e, i] = sums[i]

    def forward(j):
        number = [a <= j < b for a, b in CHUNKS].index(True)
        for step in range(1, chips):
            block = piece(2 * chip_at(chips - step) + core, j)
            if j < direct:
                arrived(block, chip_recv.at[step - 1, j])
            else:
                arrived(block, side_recv.at[step - 1, j - direct])
            if j < SIDE:
                start(block, block, side_recv.at[step - 1, SIDE - 1 - j], beside)
            start(block, block, fwd_recv.at[step - 1, number], {"ep": partner})

    order = [0] * (tp_size - 1)
    for t in range(tp_size):
        here = 1 - lax.div((tp - t) * (tp - t) + tp_size * tp_size - 1, tp_size * tp_size)
        far = sorted((o for o in range(tp_size) if o != t), key=lambda o: -abs(o - t))
        order = [k + here * ((o - t) % tp_size) for k, o in zip(order, far)]
    order.append(0)

    def own(k):
        return isinstance(k, int)

    def project(step, group):
        index = chip_at(step)
        both = jnp.concatenate([hidden[2 * index + 1 - core], hidden[2 * index + core]], axis=0)
        for k in group:
            columns = pl.ds(pl.multiple_of(tp_at(k) * out_width, out_width), out_width)
            out = jnp.dot(both, down_buf[:, columns], preferred_element_type=F32)
            core_out[step, k] = out[:toks].astype(BF16)
            core_sum[step, k] = out[toks:]
        for k in group:
            start(
                core_out.at[step, k],
                core_in.at[step, k],
                core_recv.at[step, k],
                {"ep": partner},
            )

    def crossed(step, k):
        block = core_in.at[step, k]
        arrived(block, core_recv.at[step, k])
        return core_sum[step, k] + block[...].astype(F32)

    def own_chip(k):
        total = crossed(0, k)
        own_sum[k] = total[:, :cut]
        if not own(k):
            early_out[k - 1] = total[:, cut:].astype(BF16)
            start(early_out.at[k - 1], early_in.at[k - 1], early_recv, {"tp": tp_at(k)})
        else:
            near_sum[...] = total[:, cut:]

    def send_chip(step, k):
        slot = step - 1
        start(
            chip_out.at[k, slot],
            chip_in.at[k, slot],
            red_recv.at[k, slot],
            {"ep": 2 * chip_at(step) + core},
            chip_sem,
        )

    def other_chip(step, k):
        total = crossed(step, k)
        slot = step - 1
        chip_out[k, slot] = total[:, :cut].astype(BF16)

        @pl.when(core == 0)
        def _():
            send_chip(step, k)

        if not own(k):
            late_out[slot, k - 1] = total[:, cut:].astype(BF16)
            start(
                late_out.at[slot, k - 1],
                late_in.at[slot, k - 1],
                late_recv.at[slot],
                {"tp": tp_at(k)},
            )
        else:
            late_sum[slot] = total[:, cut:]

    arrived(rows.at[partner], pair_recv)
    arrived(codes.at[partner], code_recv.at[0])
    mix = mixes(chip)
    for e in range(experts):
        own_expert(e, mix[e])
    forward(0)
    forward(1)
    if tp_size > 2:
        learn(0)
    loaded(down_buf, experts)
    project(0, order[: tp_size // 2])
    for j in range(2, 5):
        forward(j)
    project(0, order[tp_size // 2 :])
    for j in range(5, 8):
        forward(j)
    for j in range(8, direct):
        forward(j)
    for r in range(1, tp_size - 2):
        learn(r)
    for k in order:
        own_chip(k)
    if chips > 1:
        arrived(codes.at[pl.ds(0, ep_size - 2)], code_recv.at[1])

    for j in range(PIECES - 1, direct - 1, -1):
        forward(j)

    for step in range(1, chips):
        index = chip_at(chips - step)
        for number, (a, b) in enumerate(CHUNKS):
            first = a + odd * (PIECES - a - b)
            block = rows.at[2 * index + 1 - core, pl.ds(first, b - a)]
            arrived(block, fwd_recv.at[step - 1, number])
            if number == 0:
                mix = mixes(index)
            other_experts(index, number, mix)

        project(chips - step, order[: tp_size // 2])
        project(chips - step, order[tp_size // 2 :])

        for k in order:
            other_chip(chips - step, k)

        @pl.when(core == 0)
        def _():
            for k in order:
                src = chip_out.at[k, chips - step - 1]
                send(src, src, chip_sem, chip_sem, {"ep": partner}).wait_send()
            pl.semaphore_signal(turn, inc=1, device_id={"ep": partner}, device_id_type=MESH)

        @pl.when(core == 1)
        def _():
            pl.semaphore_wait(turn, 1)
            for k in order:
                send_chip(chips - step, k)


    def reduced(k):
        total = own_sum[k]
        for slot in range(chips - 1):
            block = chip_in.at[k, slot]
            arrived(block, red_recv.at[k, slot])
            total = total + block[...].astype(F32)
        return total

    def own_features(k):
        feat_out[k - 1] = reduced(k).astype(BF16)
        start(feat_out.at[k - 1], feat_in.at[k - 1], feat_recv, {"tp": tp_at(k)})

    for k in order[:-2]:
        own_features(k)

    def add_late():
        for slot in range(chips - 1):
            total = late_sum[slot]
            arrived(late_in.at[slot], late_recv.at[slot])
            for k in range(1, tp_size):
                total = total + late_in[slot, k - 1].astype(F32)
            back_out[slot] = total.astype(BF16)
            start(
                back_out.at[slot],
                back_in.at[slot],
                back_recv,
                {"ep": 2 * chip_at(slot + 1) + core},
            )

    marked = len(sent)

    @pl.when(tp < tp_size // 2)
    def _():
        own_features(order[-2])
        add_late()

    @pl.when(tp >= tp_size // 2)
    def _():
        add_late()
        own_features(order[-2])

    del sent[marked:]
    sent += [feat_out.at[0]] + [back_out.at[slot] for slot in range(chips - 1)]
    left = reduced(0)
    right = near_sum[...]
    arrived(early_in, early_recv)
    for k in range(1, tp_size):
        right = right + early_in[k - 1].astype(F32)
    arrived(feat_in, feat_recv)
    for k in range(1, tp_size):
        left = left + feat_in[k - 1].astype(F32)
    if chips > 1:
        arrived(back_in, back_recv)
    for slot in range(chips - 1):
        right = right + back_in[slot].astype(F32)
    mixed = jnp.concatenate([left, right], axis=1)

    squares = mixed * mixed
    folded = jnp.zeros((toks, LANES), F32)
    for j in range(out_width // LANES):
        folded = folded + squares[:, j * LANES : (j + 1) * LANES]
    wide = square_out.shape[1]
    if wide > toks:
        folded = jnp.concatenate([folded, jnp.zeros((wide - toks, LANES), F32)], axis=0)
    line = jnp.sum(folded.T, axis=0, keepdims=True)
    square_out[...] = jnp.broadcast_to(line, square_out.shape)
    for k in range(1, tp_size):
        start(square_out, square_in.at[k - 1], sq_recv, {"tp": tp_at(k)})
    arrived(square_in, sq_recv)
    for k in range(1, tp_size):
        line = line + square_in[k - 1, 0:1, :]
    total = jnp.broadcast_to(line, (LANES, wide)).T[:toks, :1]
    factor = lax.rsqrt(total / width + EPS)
    smalls[4].wait()
    out_ref[...] = (mixed * factor * out_gain_ref[...]).astype(BF16)
    @pl.when(core == 1)
    def _():
        for step in range(1, chips):
            for k in order:
                src = chip_out.at[k, step - 1]
                send(src, src, chip_sem, chip_sem, {"ep": partner}).wait_send()

    for src in sent:
        send(src, src, sent_sem, sent_sem, {"ep": partner}).wait_send()


def on_device(
    tokens, routing, route_weight, norm_gain, gate_weight, up_weight, down_weight, out_gain
):
    toks, width = tokens.shape
    experts, _, ff = gate_weight.shape
    ep_size, tp_size = lax.axis_size("ep"), lax.axis_size("tp")
    chips = ep_size // 2
    wide = pl.cdiv(toks, LANES) * LANES
    out_width = width // tp_size
    cut = out_width // 2
    vmem = pl.BlockSpec(memory_space=pltpu.VMEM)
    hbm = pl.BlockSpec(memory_space=pl.ANY)
    dma = pltpu.SemaphoreType.DMA
    return pl.pallas_call(
        functools.partial(kernel, ep_size, tp_size),
        out_shape=pltpu.VMEM((toks, out_width), BF16),
        in_specs=[hbm] * 8,
        out_specs=vmem,
        scratch_shapes=[
            pltpu.VMEM(tokens.shape, tokens.dtype),
            pltpu.VMEM(routing.shape[::-1], routing.dtype),
            pltpu.VMEM(routing.shape[::-1], F32),
            pltpu.VMEM((1, width), F32),
            pltpu.VMEM((1, out_width), F32),
            pltpu.VMEM((ep_size, PIECES, toks, width // PIECES), BF16),
            pltpu.VMEM((ep_size, pl.cdiv(experts * ep_size, 8) * 8, wide), F32),
            pltpu.VMEM((experts, 2, width, ff), BF16),
            pltpu.VMEM((experts * ff, width), BF16),
            pltpu.VMEM((experts, 2, 2 * toks, ff), F32),
            pltpu.VMEM((ep_size, toks, experts * ff), BF16),
            pltpu.VMEM((chips, tp_size, toks, out_width), BF16),
            pltpu.VMEM((chips, tp_size, toks, out_width), BF16),
            pltpu.VMEM((chips, tp_size, toks, out_width), F32),
            pltpu.VMEM((tp_size, toks, cut), F32),
            pltpu.VMEM((toks, cut), F32),
            pltpu.VMEM((chips - 1, toks, cut), F32),
            pltpu.VMEM((tp_size, chips - 1, toks, cut), BF16),
            pltpu.VMEM((tp_size, chips - 1, toks, cut), BF16),
            pltpu.VMEM((tp_size - 1, toks, cut), BF16),
            pltpu.VMEM((tp_size - 1, toks, cut), BF16),
            pltpu.VMEM((chips - 1, tp_size - 1, toks, cut), BF16),
            pltpu.VMEM((chips - 1, tp_size - 1, toks, cut), BF16),
            pltpu.VMEM((chips - 1, toks, cut), BF16),
            pltpu.VMEM((chips - 1, toks, cut), BF16),
            pltpu.VMEM((tp_size - 1, toks, cut), BF16),
            pltpu.VMEM((tp_size - 1, toks, cut), BF16),
            pltpu.VMEM((8, wide), F32),
            pltpu.VMEM((tp_size - 1, 8, wide), F32),
            dma((5,)),
            dma((experts + 1,)),
            pltpu.SemaphoreType.REGULAR((tp_size - 2,)),
            pltpu.SemaphoreType.REGULAR,
            dma,
            dma,
            dma,
            dma((2,)),
            dma((chips - 1, PIECES - SIDE)),
            dma((chips - 1, SIDE)),
            dma((chips - 1, len(CHUNKS))),
            dma((chips, tp_size)),
            dma((tp_size, chips - 1)),
            dma,
            dma((chips - 1,)),
            dma,
            dma,
            dma,
        ],
        compiler_params=pltpu.CompilerParams(
            collective_id=0, has_side_effects=True, vmem_limit_bytes=60 * 1024 * 1024
        ),
    )(
        tokens,
        routing.T,
        route_weight.T,
        norm_gain.reshape(1, width),
        out_gain.reshape(1, out_width),
        gate_weight,
        up_weight,
        down_weight,
    )


def solution(mesh):
    in_specs = (
        P(("grp", "ep"), None),
        P(("grp", "ep"), None),
        P(("grp", "ep"), None),
        P(),
        P("ep", None, "tp"),
        P("ep", None, "tp"),
        P("ep", "tp", None),
        P("tp"),
    )
    out_specs = P(("grp", "ep"), "tp")
    return jax.shard_map(
        on_device, mesh=mesh, in_specs=in_specs, out_specs=out_specs, check_vma=False
    )
```

```python
import functools

import jax
import jax.numpy as jnp
from jax import lax
from jax.experimental import pallas as pl
from jax.experimental.pallas import tpu as pltpu
from jax.sharding import PartitionSpec as P

LIMIT = 7.0
ALPHA = 1.702
EPS = 1e-06
LANES = 128
PIECES = 16
SIDE = 4
CHUNKS = ((0, 8), (8, 12), (12, 16))
GROUPS = ((0, 1), (1, 1), (2, 1), (3, 1), (4, 4), (8, 4))
MESH = pl.DeviceIdType.MESH
BF16 = jnp.bfloat16
F32 = jnp.float32


def kernel(
    ep_size,
    tp_size,
    tok_hbm,
    route_hbm,
    weight_hbm,
    gain_hbm,
    out_gain_hbm,
    gate_hbm,
    up_hbm,
    down_hbm,
    out_ref,
    tok_ref,
    route_ref,
    weight_ref,
    gain_ref,
    out_gain_ref,
    rows,
    codes,
    gu_buf,
    down_buf,
    acc,
    hidden,
    core_out,
    core_in,
    core_sum,
    own_sum,
    near_sum,
    late_sum,
    chip_out,
    chip_in,
    early_out,
    early_in,
    late_out,
    late_in,
    back_out,
    back_in,
    feat_out,
    feat_in,
    square_out,
    square_in,
    small_sem,
    load_sem,
    ready,
    turn,
    sent_sem,
    chip_sem,
    pair_recv,
    code_recv,
    chip_recv,
    side_recv,
    fwd_recv,
    own_recv,
    core_recv,
    red_recv,
    early_recv,
    late_recv,
    back_recv,
    feat_recv,
    sq_recv,
):
    me, tp = lax.axis_index("ep"), lax.axis_index("tp")
    core = lax.rem(me, 2)
    chip = lax.div(me, 2)
    odd = lax.rem(tp, 2)
    partner = me + 1 - 2 * core
    beside = {"tp": tp + 1 - 2 * odd}
    chips = ep_size // 2
    toks, width = tok_ref.shape
    experts, _, _, ff = gu_buf.shape
    out_width = width // tp_size
    cut = out_width // 2
    depth = width // PIECES

    chip_table = [lax.rem(chip + step, chips) for step in range(chips)]

    def chip_at(step):
        return chip_table[step]

    def tp_at(step):
        return lax.rem(tp + step, tp_size)

    def send(src, dst, send_sem, recv_sem, device):
        return pltpu.make_async_remote_copy(
            src_ref=src,
            dst_ref=dst,
            send_sem=send_sem,
            recv_sem=recv_sem,
            device_id=device,
            device_id_type=MESH,
        )

    sent = []

    def start(src, dst, recv_sem, device, out_sem=sent_sem):
        copy = send(src, dst, out_sem, recv_sem, device)
        copy.start()
        if out_sem is sent_sem:
            sent.append(src)

    def arrived(slot, sem):
        send(slot, slot, sent_sem, sem, {"ep": partner}).wait_recv()

    def tell(sem):
        @pl.when(tp > 0)
        def _():
            pl.semaphore_signal(sem, inc=1, device_id={"tp": tp - 1}, device_id_type=MESH)

        @pl.when(tp < tp_size - 1)
        def _():
            pl.semaphore_signal(sem, inc=1, device_id={"tp": tp + 1}, device_id_type=MESH)

    def learn(r):
        pl.semaphore_wait(ready.at[r], beside_count)
        if r + 1 < tp_size - 2:
            tell(ready.at[r + 1])

    beside_count = lax.div(tp + tp_size - 1, tp_size) + lax.div(2 * tp_size - 2 - tp, tp_size)

    loads = []
    for e in range(experts):
        loads.append((gate_hbm.at[e], gu_buf.at[e, 0], e))
        loads.append((up_hbm.at[e], gu_buf.at[e, 1], e))
    for e in range(experts):
        loads.append((down_hbm.at[e], down_buf.at[pl.ds(e * ff, ff)], experts))
    loads = [pltpu.make_async_copy(src, dst, load_sem.at[i]) for src, dst, i in loads]

    def loaded(slot, i):
        pltpu.make_async_copy(slot, slot, load_sem.at[i]).wait()

    smalls = (
        (tok_hbm, tok_ref),
        (gain_hbm, gain_ref),
        (route_hbm, route_ref),
        (weight_hbm, weight_ref),
        (out_gain_hbm, out_gain_ref),
    )
    smalls = [
        pltpu.make_async_copy(src, dst, small_sem.at[i]) for i, (src, dst) in enumerate(smalls)
    ]
    barrier = pltpu.get_barrier_semaphore()
    for load in smalls:
        load.start()
    for step in range(1, ep_size):
        pl.semaphore_signal(
            barrier, inc=1, device_id={"ep": lax.rem(me + step, ep_size)}, device_id_type=MESH
        )
    tell(barrier)
    for load in loads:
        load.start()

    for load in smalls[:2]:
        load.wait()
    scaled = tok_ref[...].astype(F32)
    scale = lax.rsqrt(jnp.mean(scaled * scaled, axis=-1, keepdims=True) + EPS)
    scaled = (scaled * scale * gain_ref[...]).astype(BF16)
    for p in range(PIECES):
        rows[me, p] = scaled[:, p * depth : (p + 1) * depth]

    pl.semaphore_wait(barrier, ep_size - 1 + beside_count)

    def pieces(slot, first, count):
        return rows.at[slot, pl.ds(first + odd * (PIECES - 2 * first - count), count)]

    start(rows.at[me], rows.at[me], pair_recv, {"ep": partner})
    for g, (first, count) in enumerate(GROUPS):
        for step in range(1, chips):
            block = pieces(me, first, count)
            start(block, block, chip_recv.at[step - 1, g], {"ep": 2 * chip_at(step) + core})

    if tp_size > 2:
        tell(ready.at[0])

    for load in smalls[2:4]:
        load.wait()
    place = lax.broadcasted_iota(jnp.int32, (codes.shape[1], toks), 0)
    placed = jnp.zeros(place.shape, F32)
    for k in range(route_ref.shape[0]):
        placed = placed + jnp.where(place == route_ref[k : k + 1], weight_ref[k : k + 1], 0.0)
    codes[me] = jnp.zeros(codes.shape[1:], F32)
    codes[me, :, :toks] = placed
    start(codes.at[me], codes.at[me], code_recv.at[0], {"ep": partner})
    for step in range(1, chips):
        for other in range(2):
            start(
                codes.at[me],
                codes.at[me],
                code_recv.at[1],
                {"ep": 2 * chip_at(step) + other},
            )

    def mixes(index):
        columns = jnp.concatenate([codes[2 * index + c].T[:toks] for c in range(2)], axis=0)
        lane = lax.broadcasted_iota(jnp.int32, columns.shape, 1)
        return [
            jnp.sum(jnp.where(lane == me * experts + e, columns, 0.0), axis=1, keepdims=True)
            for e in range(experts)
        ]

    def features(index, first, count):
        both = pl.ds(2 * index, 2)
        parts = [rows[both, first + t].reshape(2 * toks, depth) for t in range(count)]
        return jnp.concatenate(parts, axis=1)

    def activate(index, e, gate, up, mix):
        gate = jnp.minimum(gate, LIMIT)
        up = jnp.clip(up, -LIMIT, LIMIT)
        act = (up + 1.0) * gate * jax.nn.sigmoid(ALPHA * gate) * mix
        act = act.astype(BF16).reshape(2, toks, ff)
        hidden[pl.ds(2 * index, 2), :, e * ff : (e + 1) * ff] = act

    def own_expert(e, mix):
        x = features(chip, 0, PIECES)
        loaded(gu_buf.at[e], e)
        gate = jnp.dot(x, gu_buf[e, 0], preferred_element_type=F32)
        up = jnp.dot(x, gu_buf[e, 1], preferred_element_type=F32)
        activate(chip, e, gate, up, mix)

    def other_experts(index, number, mix):
        a, b = CHUNKS[number]
        first = a + odd * (PIECES - a - b)
        x = features(index, first, b - a)
        part = pl.ds(pl.multiple_of(first * depth, depth), (b - a) * depth)
        for e in range(experts):
            sums = []
            for i in range(2):
                total = jnp.dot(x, gu_buf[e, i, part, :], preferred_element_type=F32)
                if number:
                    total = total + acc[e, i]
                sums.append(total)
            if number == len(CHUNKS) - 1:
                activate(index, e, sums[0], sums[1], mix[e])
            else:
                for i in range(2):
                    acc[e, i] = sums[i]

    def forward(g):
        first, count = GROUPS[g] if g < len(GROUPS) else (PIECES - SIDE, SIDE)
        number = [a <= first < b for a, b in CHUNKS].index(True)
        for step in range(1, chips):
            block = pieces(2 * chip_at(chips - step) + core, first, count)
            if g < len(GROUPS):
                arrived(block, chip_recv.at[step - 1, g])
            else:
                arrived(block, side_recv.at[step - 1])
            if g < SIDE:
                start(block, block, side_recv.at[step - 1], beside)
            start(block, block, fwd_recv.at[step - 1, number], {"ep": partner})

    order = [0] * (tp_size - 1)
    for t in range(tp_size):
        here = 1 - lax.div((tp - t) * (tp - t) + tp_size * tp_size - 1, tp_size * tp_size)
        far = sorted((o for o in range(tp_size) if o != t), key=lambda o: -abs(o - t))
        order = [k + here * ((o - t) % tp_size) for k, o in zip(order, far)]
    order.append(0)

    def own(k):
        return isinstance(k, int)

    def project(step, group):
        index = chip_at(step)
        both = jnp.concatenate([hidden[2 * index + 1 - core], hidden[2 * index + core]], axis=0)
        for k in group:
            columns = pl.ds(pl.multiple_of(tp_at(k) * out_width, out_width), out_width)
            out = jnp.dot(both, down_buf[:, columns], preferred_element_type=F32)
            core_out[step, k] = out[:toks].astype(BF16)
            core_sum[step, k] = out[toks:]
        for k in group:
            start(
                core_out.at[step, k],
                core_in.at[step, k],
                core_recv.at[step - 1, k] if step else own_recv,
                {"ep": partner},
            )

    def crossed(step, k):
        if step:
            arrived(core_in.at[step, k], core_recv.at[step - 1, k])
        return core_sum[step, k] + core_in[step, k].astype(F32)

    def own_chip(k):
        total = crossed(0, k)
        own_sum[k] = total[:, :cut]
        if not own(k):
            early_out[k - 1] = total[:, cut:].astype(BF16)
            start(early_out.at[k - 1], early_in.at[k - 1], early_recv, {"tp": tp_at(k)})
        else:
            near_sum[...] = total[:, cut:]

    def send_chip(step, k):
        slot = step - 1
        start(
            chip_out.at[k, slot],
            chip_in.at[k, slot],
            red_recv.at[k, slot],
            {"ep": 2 * chip_at(step) + core},
            chip_sem,
        )

    def other_chip(step, k):
        total = crossed(step, k)
        slot = step - 1
        chip_out[k, slot] = total[:, :cut].astype(BF16)

        @pl.when(core == 0)
        def _():
            send_chip(step, k)

        if not own(k):
            late_out[slot, k - 1] = total[:, cut:].astype(BF16)
            start(
                late_out.at[slot, k - 1],
                late_in.at[slot, k - 1],
                late_recv.at[slot],
                {"tp": tp_at(k)},
            )
        else:
            late_sum[slot] = total[:, cut:]

    arrived(rows.at[partner], pair_recv)
    arrived(codes.at[partner], code_recv.at[0])
    mix = mixes(chip)
    for e in range(experts):
        own_expert(e, mix[e])
    forward(0)
    forward(1)
    if tp_size > 2:
        learn(0)
    loaded(down_buf, experts)
    project(0, order[: tp_size // 2])
    forward(2)
    forward(3)
    project(0, order[tp_size // 2 :])
    forward(4)
    for r in range(1, tp_size - 2):
        learn(r)
    forward(5)
    arrived(core_in.at[0], own_recv)
    for k in order:
        own_chip(k)
    if chips > 1:
        arrived(codes.at[pl.ds(0, ep_size - 2)], code_recv.at[1])
    forward(6)
    for step in range(1, chips):
        index = chip_at(chips - step)
        for number, (a, b) in enumerate(CHUNKS):
            first = a + odd * (PIECES - a - b)
            block = rows.at[2 * index + 1 - core, pl.ds(first, b - a)]
            arrived(block, fwd_recv.at[step - 1, number])
            if number == 0:
                mix = mixes(index)
            other_experts(index, number, mix)

        for k in order:
            project(chips - step, [k])

        for k in order:
            other_chip(chips - step, k)

        @pl.when(core == 0)
        def _():
            for k in order[:3]:
                src = chip_out.at[k, chips - step - 1]
                send(src, src, chip_sem, chip_sem, {"ep": partner}).wait_send()
            pl.semaphore_signal(turn, inc=1, device_id={"ep": partner}, device_id_type=MESH)

        @pl.when(core == 1)
        def _():
            pl.semaphore_wait(turn, 1)
            for k in order:
                send_chip(chips - step, k)


    def reduced(k):
        total = own_sum[k]
        for slot in range(chips - 1):
            block = chip_in.at[k, slot]
            arrived(block, red_recv.at[k, slot])
            total = total + block[...].astype(F32)
        return total

    def own_features(k):
        feat_out[k - 1] = reduced(k).astype(BF16)
        start(feat_out.at[k - 1], feat_in.at[k - 1], feat_recv, {"tp": tp_at(k)})

    for k in order[:-2]:
        own_features(k)

    def add_late():
        for slot in range(chips - 1):
            total = late_sum[slot]
            arrived(late_in.at[slot], late_recv.at[slot])
            for k in range(1, tp_size):
                total = total + late_in[slot, k - 1].astype(F32)
            back_out[slot] = total.astype(BF16)
            start(
                back_out.at[slot],
                back_in.at[slot],
                back_recv,
                {"ep": 2 * chip_at(slot + 1) + core},
            )

    own_features(order[-2])
    add_late()
    left = reduced(0)
    right = near_sum[...]
    arrived(early_in, early_recv)
    for k in range(1, tp_size):
        right = right + early_in[k - 1].astype(F32)
    arrived(feat_in, feat_recv)
    for k in range(1, tp_size):
        left = left + feat_in[k - 1].astype(F32)
    if chips > 1:
        arrived(back_in, back_recv)
    for slot in range(chips - 1):
        right = right + back_in[slot].astype(F32)
    mixed = jnp.concatenate([left, right], axis=1)

    squares = mixed * mixed
    folded = jnp.zeros((toks, LANES), F32)
    for j in range(out_width // LANES):
        folded = folded + squares[:, j * LANES : (j + 1) * LANES]
    wide = square_out.shape[1]
    if wide > toks:
        folded = jnp.concatenate([folded, jnp.zeros((wide - toks, LANES), F32)], axis=0)
    line = jnp.sum(folded.T, axis=0, keepdims=True)
    square_out[...] = jnp.broadcast_to(line, square_out.shape)
    for k in range(1, tp_size):
        start(square_out, square_in.at[k - 1], sq_recv, {"tp": tp_at(k)})
    arrived(square_in, sq_recv)
    for k in range(1, tp_size):
        line = line + square_in[k - 1, 0:1, :]
    total = jnp.broadcast_to(line, (LANES, wide)).T[:toks, :1]
    factor = lax.rsqrt(total / width + EPS)
    smalls[4].wait()
    out_ref[...] = (mixed * factor * out_gain_ref[...]).astype(BF16)
    def left_over(ks):
        for step in range(1, chips):
            for k in ks:
                src = chip_out.at[k, step - 1]
                send(src, src, chip_sem, chip_sem, {"ep": partner}).wait_send()

    @pl.when(core == 1)
    def _():
        left_over(order)

    @pl.when(core == 0)
    def _():
        left_over(order[3:])

    for src in sent:
        send(src, src, sent_sem, sent_sem, {"ep": partner}).wait_send()


def on_device(
    tokens, routing, route_weight, norm_gain, gate_weight, up_weight, down_weight, out_gain
):
    toks, width = tokens.shape
    experts, _, ff = gate_weight.shape
    ep_size, tp_size = lax.axis_size("ep"), lax.axis_size("tp")
    chips = ep_size // 2
    wide = pl.cdiv(toks, LANES) * LANES
    out_width = width // tp_size
    cut = out_width // 2
    vmem = pl.BlockSpec(memory_space=pltpu.VMEM)
    hbm = pl.BlockSpec(memory_space=pl.ANY)
    dma = pltpu.SemaphoreType.DMA
    return pl.pallas_call(
        functools.partial(kernel, ep_size, tp_size),
        out_shape=pltpu.VMEM((toks, out_width), BF16),
        in_specs=[hbm] * 8,
        out_specs=vmem,
        scratch_shapes=[
            pltpu.VMEM(tokens.shape, tokens.dtype),
            pltpu.VMEM(routing.shape[::-1], routing.dtype),
            pltpu.VMEM(routing.shape[::-1], F32),
            pltpu.VMEM((1, width), F32),
            pltpu.VMEM((1, out_width), F32),
            pltpu.VMEM((ep_size, PIECES, toks, width // PIECES), BF16),
            pltpu.VMEM((ep_size, pl.cdiv(experts * ep_size, 8) * 8, wide), F32),
            pltpu.VMEM((experts, 2, width, ff), BF16),
            pltpu.VMEM((experts * ff, width), BF16),
            pltpu.VMEM((experts, 2, 2 * toks, ff), F32),
            pltpu.VMEM((ep_size, toks, experts * ff), BF16),
            pltpu.VMEM((chips, tp_size, toks, out_width), BF16),
            pltpu.VMEM((chips, tp_size, toks, out_width), BF16),
            pltpu.VMEM((chips, tp_size, toks, out_width), F32),
            pltpu.VMEM((tp_size, toks, cut), F32),
            pltpu.VMEM((toks, cut), F32),
            pltpu.VMEM((chips - 1, toks, cut), F32),
            pltpu.VMEM((tp_size, chips - 1, toks, cut), BF16),
            pltpu.VMEM((tp_size, chips - 1, toks, cut), BF16),
            pltpu.VMEM((tp_size - 1, toks, cut), BF16),
            pltpu.VMEM((tp_size - 1, toks, cut), BF16),
            pltpu.VMEM((chips - 1, tp_size - 1, toks, cut), BF16),
            pltpu.VMEM((chips - 1, tp_size - 1, toks, cut), BF16),
            pltpu.VMEM((chips - 1, toks, cut), BF16),
            pltpu.VMEM((chips - 1, toks, cut), BF16),
            pltpu.VMEM((tp_size - 1, toks, cut), BF16),
            pltpu.VMEM((tp_size - 1, toks, cut), BF16),
            pltpu.VMEM((8, wide), F32),
            pltpu.VMEM((tp_size - 1, 8, wide), F32),
            dma((5,)),
            dma((experts + 1,)),
            pltpu.SemaphoreType.REGULAR((tp_size - 2,)),
            pltpu.SemaphoreType.REGULAR,
            dma,
            dma,
            dma,
            dma((2,)),
            dma((chips - 1, len(GROUPS))),
            dma((chips - 1,)),
            dma((chips - 1, len(CHUNKS))),
            dma,
            dma((chips - 1, tp_size)),
            dma((tp_size, chips - 1)),
            dma,
            dma((chips - 1,)),
            dma,
            dma,
            dma,
        ],
        compiler_params=pltpu.CompilerParams(
            collective_id=0, has_side_effects=True, vmem_limit_bytes=60 * 1024 * 1024
        ),
    )(
        tokens,
        routing.T,
        route_weight.T,
        norm_gain.reshape(1, width),
        out_gain.reshape(1, out_width),
        gate_weight,
        up_weight,
        down_weight,
    )


def solution(mesh):
    in_specs = (
        P(("grp", "ep"), None),
        P(("grp", "ep"), None),
        P(("grp", "ep"), None),
        P(),
        P("ep", None, "tp"),
        P("ep", None, "tp"),
        P("ep", "tp", None),
        P("tp"),
    )
    out_specs = P(("grp", "ep"), "tp")
    return jax.shard_map(
        on_device, mesh=mesh, in_specs=in_specs, out_specs=out_specs, check_vma=False
    )
```

```python
import functools

import jax
import jax.numpy as jnp
from jax import lax
from jax.experimental import pallas as pl
from jax.experimental.pallas import tpu as pltpu
from jax.sharding import PartitionSpec as P

LIMIT = 7.0
ALPHA = 1.702
EPS = 1e-06
LANES = 128
PIECES = 16
SIDE = 4
CHUNKS = ((0, 8), (8, 12), (12, 16))
GROUPS = ((0, 1), (1, 1), (2, 1), (3, 1), (4, 4), (8, 4))
MESH = pl.DeviceIdType.MESH
BF16 = jnp.bfloat16
F32 = jnp.float32


def kernel(
    ep_size,
    tp_size,
    tok_hbm,
    route_hbm,
    weight_hbm,
    gain_hbm,
    out_gain_hbm,
    gate_hbm,
    up_hbm,
    down_hbm,
    out_ref,
    tok_ref,
    route_ref,
    weight_ref,
    gain_ref,
    out_gain_ref,
    rows,
    codes,
    gu_buf,
    down_buf,
    acc,
    hidden,
    core_out,
    core_in,
    core_sum,
    own_sum,
    near_sum,
    late_sum,
    chip_out,
    chip_in,
    early_out,
    early_in,
    late_out,
    late_in,
    back_out,
    back_in,
    feat_out,
    feat_in,
    square_out,
    square_in,
    small_sem,
    load_sem,
    ready,
    turn,
    sent_sem,
    chip_sem,
    pair_recv,
    code_recv,
    chip_recv,
    side_recv,
    fwd_recv,
    own_recv,
    core_recv,
    red_recv,
    early_recv,
    late_recv,
    back_recv,
    feat_recv,
    sq_recv,
):
    me, tp = lax.axis_index("ep"), lax.axis_index("tp")
    core = lax.rem(me, 2)
    chip = lax.div(me, 2)
    odd = lax.rem(tp, 2)
    partner = me + 1 - 2 * core
    beside = {"tp": tp + 1 - 2 * odd}
    chips = ep_size // 2
    toks, width = tok_ref.shape
    experts, _, _, ff = gu_buf.shape
    out_width = width // tp_size
    cut = out_width // 2
    depth = width // PIECES

    chip_table = [lax.rem(chip + step, chips) for step in range(chips)]

    def chip_at(step):
        return chip_table[step]

    def tp_at(step):
        return lax.rem(tp + step, tp_size)

    def send(src, dst, send_sem, recv_sem, device):
        return pltpu.make_async_remote_copy(
            src_ref=src,
            dst_ref=dst,
            send_sem=send_sem,
            recv_sem=recv_sem,
            device_id=device,
            device_id_type=MESH,
        )

    sent = []

    def start(src, dst, recv_sem, device, out_sem=sent_sem):
        copy = send(src, dst, out_sem, recv_sem, device)
        copy.start()
        if out_sem is sent_sem:
            sent.append(src)

    def arrived(slot, sem):
        send(slot, slot, sent_sem, sem, {"ep": partner}).wait_recv()

    def tell(sem):
        @pl.when(tp > 0)
        def _():
            pl.semaphore_signal(sem, inc=1, device_id={"tp": tp - 1}, device_id_type=MESH)

        @pl.when(tp < tp_size - 1)
        def _():
            pl.semaphore_signal(sem, inc=1, device_id={"tp": tp + 1}, device_id_type=MESH)

    def learn(r):
        pl.semaphore_wait(ready.at[r], beside_count)
        if r + 1 < tp_size - 2:
            tell(ready.at[r + 1])

    beside_count = lax.div(tp + tp_size - 1, tp_size) + lax.div(2 * tp_size - 2 - tp, tp_size)

    loads = []
    for e in range(experts):
        loads.append((gate_hbm.at[e], gu_buf.at[e, 0], e))
        loads.append((up_hbm.at[e], gu_buf.at[e, 1], e))
    for e in range(experts):
        loads.append((down_hbm.at[e], down_buf.at[pl.ds(e * ff, ff)], experts))
    loads = [pltpu.make_async_copy(src, dst, load_sem.at[i]) for src, dst, i in loads]

    def loaded(slot, i):
        pltpu.make_async_copy(slot, slot, load_sem.at[i]).wait()

    smalls = (
        (tok_hbm, tok_ref),
        (gain_hbm, gain_ref),
        (route_hbm, route_ref),
        (weight_hbm, weight_ref),
        (out_gain_hbm, out_gain_ref),
    )
    smalls = [
        pltpu.make_async_copy(src, dst, small_sem.at[i]) for i, (src, dst) in enumerate(smalls)
    ]
    barrier = pltpu.get_barrier_semaphore()
    for load in smalls:
        load.start()
    for step in range(1, ep_size):
        pl.semaphore_signal(
            barrier, inc=1, device_id={"ep": lax.rem(me + step, ep_size)}, device_id_type=MESH
        )
    tell(barrier)
    for load in loads:
        load.start()

    for load in smalls[:2]:
        load.wait()
    scaled = tok_ref[...].astype(F32)
    scale = lax.rsqrt(jnp.mean(scaled * scaled, axis=-1, keepdims=True) + EPS)
    scaled = (scaled * scale * gain_ref[...]).astype(BF16)
    for p in range(PIECES):
        rows[me, p] = scaled[:, p * depth : (p + 1) * depth]

    pl.semaphore_wait(barrier, ep_size - 1 + beside_count)

    def pieces(slot, first, count):
        return rows.at[slot, pl.ds(first + odd * (PIECES - 2 * first - count), count)]

    start(rows.at[me], rows.at[me], pair_recv, {"ep": partner})
    for g, (first, count) in enumerate(GROUPS):
        for step in range(1, chips):
            block = pieces(me, first, count)
            start(block, block, chip_recv.at[step - 1, g], {"ep": 2 * chip_at(step) + core})

    if tp_size > 2:
        tell(ready.at[0])

    for load in smalls[2:4]:
        load.wait()
    place = lax.broadcasted_iota(jnp.int32, (codes.shape[1], toks), 0)
    placed = jnp.zeros(place.shape, F32)
    for k in range(route_ref.shape[0]):
        placed = placed + jnp.where(place == route_ref[k : k + 1], weight_ref[k : k + 1], 0.0)
    codes[me] = jnp.zeros(codes.shape[1:], F32)
    codes[me, :, :toks] = placed
    start(codes.at[me], codes.at[me], code_recv.at[0], {"ep": partner})
    for step in range(1, chips):
        for other in range(2):
            start(
                codes.at[me],
                codes.at[me],
                code_recv.at[1],
                {"ep": 2 * chip_at(step) + other},
            )

    def mixes(index):
        columns = jnp.concatenate([codes[2 * index + c].T[:toks] for c in range(2)], axis=0)
        lane = lax.broadcasted_iota(jnp.int32, columns.shape, 1)
        return [
            jnp.sum(jnp.where(lane == me * experts + e, columns, 0.0), axis=1, keepdims=True)
            for e in range(experts)
        ]

    def features(index, first, count):
        both = pl.ds(2 * index, 2)
        parts = [rows[both, first + t].reshape(2 * toks, depth) for t in range(count)]
        return jnp.concatenate(parts, axis=1)

    def activate(index, e, gate, up, mix):
        gate = jnp.minimum(gate, LIMIT)
        up = jnp.clip(up, -LIMIT, LIMIT)
        act = (up + 1.0) * gate * jax.nn.sigmoid(ALPHA * gate) * mix
        act = act.astype(BF16).reshape(2, toks, ff)
        hidden[pl.ds(2 * index, 2), :, e * ff : (e + 1) * ff] = act

    def own_expert(e, mix):
        x = features(chip, 0, PIECES)
        loaded(gu_buf.at[e], e)
        gate = jnp.dot(x, gu_buf[e, 0], preferred_element_type=F32)
        up = jnp.dot(x, gu_buf[e, 1], preferred_element_type=F32)
        activate(chip, e, gate, up, mix)

    def other_experts(index, number, mix):
        a, b = CHUNKS[number]
        first = a + odd * (PIECES - a - b)
        x = features(index, first, b - a)
        part = pl.ds(pl.multiple_of(first * depth, depth), (b - a) * depth)
        for e in range(experts):
            sums = []
            for i in range(2):
                total = jnp.dot(x, gu_buf[e, i, part, :], preferred_element_type=F32)
                if number:
                    total = total + acc[e, i]
                sums.append(total)
            if number == len(CHUNKS) - 1:
                activate(index, e, sums[0], sums[1], mix[e])
            else:
                for i in range(2):
                    acc[e, i] = sums[i]

    def forward(g):
        first, count = GROUPS[g] if g < len(GROUPS) else (PIECES - SIDE, SIDE)
        number = [a <= first < b for a, b in CHUNKS].index(True)
        for step in range(1, chips):
            block = pieces(2 * chip_at(chips - step) + core, first, count)
            if g < len(GROUPS):
                arrived(block, chip_recv.at[step - 1, g])
            else:
                arrived(block, side_recv.at[step - 1])
            if g < SIDE:
                start(block, block, side_recv.at[step - 1], beside)
            start(block, block, fwd_recv.at[step - 1, number], {"ep": partner})

    order = [0] * (tp_size - 1)
    for t in range(tp_size):
        here = 1 - lax.div((tp - t) * (tp - t) + tp_size * tp_size - 1, tp_size * tp_size)
        far = sorted((o for o in range(tp_size) if o != t), key=lambda o: -abs(o - t))
        order = [k + here * ((o - t) % tp_size) for k, o in zip(order, far)]
    order.append(0)

    def own(k):
        return isinstance(k, int)

    def project(step, group):
        index = chip_at(step)
        both = jnp.concatenate([hidden[2 * index + 1 - core], hidden[2 * index + core]], axis=0)
        for k in group:
            columns = pl.ds(pl.multiple_of(tp_at(k) * out_width, out_width), out_width)
            out = jnp.dot(both, down_buf[:, columns], preferred_element_type=F32)
            core_out[step, k] = out[:toks].astype(BF16)
            core_sum[step, k] = out[toks:]
        for k in group:
            start(
                core_out.at[step, k],
                core_in.at[step, k],
                core_recv.at[step - 1, k] if step else own_recv,
                {"ep": partner},
            )

    def crossed(step, k):
        if step:
            arrived(core_in.at[step, k], core_recv.at[step - 1, k])
        return core_sum[step, k] + core_in[step, k].astype(F32)

    def own_chip(k):
        total = crossed(0, k)
        own_sum[k] = total[:, :cut]
        if not own(k):
            early_out[k - 1] = total[:, cut:].astype(BF16)
            start(early_out.at[k - 1], early_in.at[k - 1], early_recv, {"tp": tp_at(k)})
        else:
            near_sum[...] = total[:, cut:]

    def send_chip(step, k):
        slot = step - 1
        start(
            chip_out.at[k, slot],
            chip_in.at[k, slot],
            red_recv.at[k, slot],
            {"ep": 2 * chip_at(step) + core},
            chip_sem,
        )

    def other_chip(step, k):
        total = crossed(step, k)
        slot = step - 1
        chip_out[k, slot] = total[:, :cut].astype(BF16)

        @pl.when(core == 0)
        def _():
            send_chip(step, k)

        if not own(k):
            late_out[slot, k - 1] = total[:, cut:].astype(BF16)
            start(
                late_out.at[slot, k - 1],
                late_in.at[slot, k - 1],
                late_recv.at[slot],
                {"tp": tp_at(k)},
            )
        else:
            late_sum[slot] = total[:, cut:]

    arrived(rows.at[partner], pair_recv)
    arrived(codes.at[partner], code_recv.at[0])
    mix = mixes(chip)
    for e in range(experts):
        own_expert(e, mix[e])
    forward(0)
    forward(1)
    if tp_size > 2:
        learn(0)
    loaded(down_buf, experts)
    project(0, order[: tp_size // 2])
    forward(2)
    forward(3)
    project(0, order[tp_size // 2 :])
    forward(4)
    for r in range(1, tp_size - 2):
        learn(r)
    forward(5)
    arrived(core_in.at[0], own_recv)
    for k in order:
        own_chip(k)
    if chips > 1:
        arrived(codes.at[pl.ds(0, ep_size - 2)], code_recv.at[1])
    forward(6)
    for step in range(1, chips):
        index = chip_at(chips - step)
        for number, (a, b) in enumerate(CHUNKS):
            first = a + odd * (PIECES - a - b)
            block = rows.at[2 * index + 1 - core, pl.ds(first, b - a)]
            arrived(block, fwd_recv.at[step - 1, number])
            other_experts(index, number, None if number == 0 else mix)
            if number == 0:
                mix = mixes(index)

        for k in order:
            project(chips - step, [k])

        for k in order:
            other_chip(chips - step, k)

        @pl.when(core == 0)
        def _():
            for k in order[:3]:
                src = chip_out.at[k, chips - step - 1]
                send(src, src, chip_sem, chip_sem, {"ep": partner}).wait_send()
            pl.semaphore_signal(turn, inc=1, device_id={"ep": partner}, device_id_type=MESH)

        @pl.when(core == 1)
        def _():
            pl.semaphore_wait(turn, 1)
            for k in order:
                send_chip(chips - step, k)


    def reduced(k):
        total = own_sum[k]
        for slot in range(chips - 1):
            block = chip_in.at[k, slot]
            arrived(block, red_recv.at[k, slot])
            total = total + block[...].astype(F32)
        return total

    def own_features(k):
        feat_out[k - 1] = reduced(k).astype(BF16)
        start(feat_out.at[k - 1], feat_in.at[k - 1], feat_recv, {"tp": tp_at(k)})

    for k in order[:-2]:
        own_features(k)

    def add_late():
        for slot in range(chips - 1):
            total = late_sum[slot]
            arrived(late_in.at[slot], late_recv.at[slot])
            for k in range(1, tp_size):
                total = total + late_in[slot, k - 1].astype(F32)
            back_out[slot] = total.astype(BF16)
            start(
                back_out.at[slot],
                back_in.at[slot],
                back_recv,
                {"ep": 2 * chip_at(slot + 1) + core},
            )

    own_features(order[-2])
    add_late()
    left = reduced(0)
    right = near_sum[...]
    arrived(early_in, early_recv)
    for k in range(1, tp_size):
        right = right + early_in[k - 1].astype(F32)
    arrived(feat_in, feat_recv)
    for k in range(1, tp_size):
        left = left + feat_in[k - 1].astype(F32)
    def fold(part):
        squares = part * part
        total = squares[:, :LANES]
        for j in range(1, part.shape[1] // LANES):
            total = total + squares[:, j * LANES : (j + 1) * LANES]
        return total

    folded = fold(left)
    if chips > 1:
        arrived(back_in, back_recv)
    for slot in range(chips - 1):
        right = right + back_in[slot].astype(F32)
    folded = folded + fold(right)
    wide = square_out.shape[1]
    if wide > toks:
        folded = jnp.concatenate([folded, jnp.zeros((wide - toks, LANES), F32)], axis=0)
    line = jnp.sum(folded.T, axis=0, keepdims=True)
    square_out[...] = jnp.broadcast_to(line, square_out.shape)
    for k in range(1, tp_size):
        start(square_out, square_in.at[k - 1], sq_recv, {"tp": tp_at(k)})
    smalls[4].wait()
    mixed = jnp.concatenate([left, right], axis=1) * out_gain_ref[...]
    arrived(square_in, sq_recv)
    for k in range(1, tp_size):
        line = line + square_in[k - 1, 0:1, :]
    total = jnp.broadcast_to(line, (LANES, wide)).T[:toks, :1]
    factor = lax.rsqrt(total / width + EPS)
    out_ref[...] = (mixed * factor).astype(BF16)
    def left_over(ks):
        for step in range(1, chips):
            for k in ks:
                src = chip_out.at[k, step - 1]
                send(src, src, chip_sem, chip_sem, {"ep": partner}).wait_send()

    @pl.when(core == 1)
    def _():
        left_over(order)

    @pl.when(core == 0)
    def _():
        left_over(order[3:])

    for src in sent:
        send(src, src, sent_sem, sent_sem, {"ep": partner}).wait_send()


def on_device(
    tokens, routing, route_weight, norm_gain, gate_weight, up_weight, down_weight, out_gain
):
    toks, width = tokens.shape
    experts, _, ff = gate_weight.shape
    ep_size, tp_size = lax.axis_size("ep"), lax.axis_size("tp")
    chips = ep_size // 2
    wide = pl.cdiv(toks, LANES) * LANES
    out_width = width // tp_size
    cut = out_width // 2
    vmem = pl.BlockSpec(memory_space=pltpu.VMEM)
    hbm = pl.BlockSpec(memory_space=pl.ANY)
    dma = pltpu.SemaphoreType.DMA
    return pl.pallas_call(
        functools.partial(kernel, ep_size, tp_size),
        out_shape=pltpu.VMEM((toks, out_width), BF16),
        in_specs=[hbm] * 8,
        out_specs=vmem,
        scratch_shapes=[
            pltpu.VMEM(tokens.shape, tokens.dtype),
            pltpu.VMEM(routing.shape[::-1], routing.dtype),
            pltpu.VMEM(routing.shape[::-1], F32),
            pltpu.VMEM((1, width), F32),
            pltpu.VMEM((1, out_width), F32),
            pltpu.VMEM((ep_size, PIECES, toks, width // PIECES), BF16),
            pltpu.VMEM((ep_size, pl.cdiv(experts * ep_size, 8) * 8, wide), F32),
            pltpu.VMEM((experts, 2, width, ff), BF16),
            pltpu.VMEM((experts * ff, width), BF16),
            pltpu.VMEM((experts, 2, 2 * toks, ff), F32),
            pltpu.VMEM((ep_size, toks, experts * ff), BF16),
            pltpu.VMEM((chips, tp_size, toks, out_width), BF16),
            pltpu.VMEM((chips, tp_size, toks, out_width), BF16),
            pltpu.VMEM((chips, tp_size, toks, out_width), F32),
            pltpu.VMEM((tp_size, toks, cut), F32),
            pltpu.VMEM((toks, cut), F32),
            pltpu.VMEM((chips - 1, toks, cut), F32),
            pltpu.VMEM((tp_size, chips - 1, toks, cut), BF16),
            pltpu.VMEM((tp_size, chips - 1, toks, cut), BF16),
            pltpu.VMEM((tp_size - 1, toks, cut), BF16),
            pltpu.VMEM((tp_size - 1, toks, cut), BF16),
            pltpu.VMEM((chips - 1, tp_size - 1, toks, cut), BF16),
            pltpu.VMEM((chips - 1, tp_size - 1, toks, cut), BF16),
            pltpu.VMEM((chips - 1, toks, cut), BF16),
            pltpu.VMEM((chips - 1, toks, cut), BF16),
            pltpu.VMEM((tp_size - 1, toks, cut), BF16),
            pltpu.VMEM((tp_size - 1, toks, cut), BF16),
            pltpu.VMEM((8, wide), F32),
            pltpu.VMEM((tp_size - 1, 8, wide), F32),
            dma((5,)),
            dma((experts + 1,)),
            pltpu.SemaphoreType.REGULAR((tp_size - 2,)),
            pltpu.SemaphoreType.REGULAR,
            dma,
            dma,
            dma,
            dma((2,)),
            dma((chips - 1, len(GROUPS))),
            dma((chips - 1,)),
            dma((chips - 1, len(CHUNKS))),
            dma,
            dma((chips - 1, tp_size)),
            dma((tp_size, chips - 1)),
            dma,
            dma((chips - 1,)),
            dma,
            dma,
            dma,
        ],
        compiler_params=pltpu.CompilerParams(
            collective_id=0, has_side_effects=True, vmem_limit_bytes=60 * 1024 * 1024
        ),
    )(
        tokens,
        routing.T,
        route_weight.T,
        norm_gain.reshape(1, width),
        out_gain.reshape(1, out_width),
        gate_weight,
        up_weight,
        down_weight,
    )


def solution(mesh):
    in_specs = (
        P(("grp", "ep"), None),
        P(("grp", "ep"), None),
        P(("grp", "ep"), None),
        P(),
        P("ep", None, "tp"),
        P("ep", None, "tp"),
        P("ep", "tp", None),
        P("tp"),
    )
    out_specs = P(("grp", "ep"), "tp")
    return jax.shard_map(
        on_device, mesh=mesh, in_specs=in_specs, out_specs=out_specs, check_vma=False
    )
```
